32 devices in a mesh: ep: 8 (over z, y), tp: 4 (over x, core).
Axes of the slice: x: 2, y: 2, z: 4, core: 2. Of those that a mesh axis runs over, the one named last changes fastest.
Arguments:
- q_heads: bfloat16 [8192, 1024], P('ep', 'tp'), may hold values from -200 to 200
- k_heads: bfloat16 [8192, 256], P('ep', 'tp'), may hold values from -6 to 6
- v_heads: bfloat16 [8192, 256], P('ep', 'tp'), may hold values from -6 to 6
- sink_logits: float32 [16], P('tp'), may hold values from 1 to 5
- out_weight: bfloat16 [1024, 2048], P(None, 'tp'), may hold values from -1.5 to 1.5
- tokens_b: bfloat16 [4096, 2048], P('ep'), may hold values from -6 to 6
- moe_gain: float32 [2048], replicated, may hold values from 0.1 to 1.9
- router_group: bfloat16 [2048, 4], replicated, may hold values from -0.125 to 0.125
- router_expert: bfloat16 [2048, 16], replicated, may hold values from -0.125 to 0.125
- route_expert: int32 [4096, 2], P('ep'), may hold values from 0 to 15, as said below
- expert_gate: bfloat16 [16, 2048, 1024], P('ep', None, 'tp'), may hold values from -0.125 to 0.125
- expert_up: bfloat16 [16, 2048, 1024], P('ep', None, 'tp'), may hold values from -0.125 to 0.125
- expert_down: bfloat16 [16, 1024, 2048], P('ep', 'tp'), may hold values from -0.75 to 0.75
Outputs:
- mixer_out: bfloat16 [8192, 2048], P('ep', 'tp')
- moe_out: bfloat16 [4096, 2048], P(('ep', 'tp'))
The draws below stay inside these ranges and needn't reach their ends.
Inputs may be any that keep to these rules, and one draw needn't show every extreme that they name: `route_expert`: each token names two different experts, in rising order, of one group of 4 consecutive experts. In each aligned block of 128 rows (the rows of one device) no expert is named by more than 32 tokens, in each group one expert is named by exactly 32 tokens of every block, and each group is named by a quarter of every block's tokens.
All inputs are finite; a program needn't handle non-finite values.
Results may differ from the reference program's by a relative error of at most 0.011.
Values may be sent and summed in bfloat16 or wider, within the bound.
No kernel may reach another device: no remote copies, remote signals or barrier semaphores. Data moves between devices by JAX's collectives and lax.ppermute only.
A program may use at most 128 MiB of HBM per device.

```python
import jax
import jax.numpy as jnp
from jax import lax

D = 2048
HEADS = 16
KV = 4
HD = 64
WINDOW = 128
ROW_B = 128
GROUPS = 4
FF = 1024
EXPERTS = 16
GROUP_EXPERTS = 4
CAP = 32
TOK_A = 8192
TOK_B = 4096
N_EP = 8
N_TP = 4


def pair_heads(seed_key):
    key_query, key_keys = jax.random.split(seed_key, 2)
    group_size = HEADS // KV
    queries = jnp.clip(jax.random.normal(key_query, (TOK_A, KV, group_size, HD), jnp.float32), -5.0, 5.0)
    keys_raw = jnp.clip(jax.random.normal(key_keys, (TOK_A, KV, HD), jnp.float32), -5.0, 5.0)
    return (queries.reshape(TOK_A, HEADS * HD), keys_raw.reshape(TOK_A, KV * HD))


def draw_q_heads(key, part):
    return pair_heads(jax.random.fold_in(key, 3))[0].astype(jnp.bfloat16)


def draw_k_heads(key, part):
    return pair_heads(jax.random.fold_in(key, 3))[1].astype(jnp.bfloat16)


def draw_route_expert(key, part):
    block_count = N_EP * N_TP
    half_rows = ROW_B // 2
    quarter_rows = ROW_B // 4
    pool = jnp.repeat(jnp.arange(GROUP_EXPERTS, dtype=jnp.int32), CAP)
    favored = jax.random.randint(jax.random.fold_in(key, 7), (GROUPS,), 0, GROUP_EXPERTS)

    def one_group(group_key, group_index):
        ranks = jax.random.permutation(group_key, pool.shape[0]).astype(jnp.int32)
        ordering = jnp.where(pool == favored[group_index], -1, ranks)
        order = jnp.argsort(ordering, stable=True)
        picked = jnp.sort(pool[order[:half_rows]])
        pairs = jnp.stack([picked[:quarter_rows], picked[quarter_rows:]], axis=1)
        return pairs + group_index * GROUP_EXPERTS

    def one_block(block_key):
        group_keys = jax.random.split(block_key, GROUPS + 1)
        pairs = jax.vmap(one_group)(group_keys[:GROUPS], jnp.arange(GROUPS, dtype=jnp.int32))
        pairs = pairs.reshape(ROW_B, 2)
        return pairs[jax.random.permutation(group_keys[GROUPS], ROW_B)]
    block_keys = jax.random.split(jax.random.fold_in(key, 11), block_count)
    return jax.vmap(one_block)(block_keys).reshape(block_count * ROW_B, 2).astype(jnp.int32)


def block_levels(own_key, dims, cuts, low, largest):
    loudness, own = 1.0, jax.random.fold_in(own_key, 6)
    for axis_at, shards_of in cuts:
        heights = jnp.exp(jax.random.uniform(jax.random.fold_in(own, axis_at), (shards_of,), jnp.float32, low / len(cuts), largest / len(cuts)))
        loudness = loudness * jnp.repeat(heights, dims[axis_at] // shards_of).reshape([-1 if axis == axis_at else 1 for axis in range(len(dims))])
    return loudness


def scatter_about(key, dims, spread, limit, cuts=(), held_as=jnp.bfloat16):
    result = spread * jax.random.normal(key, dims, jnp.float32)
    if cuts:
        result = result * block_levels(key, dims, cuts, -0.22, 0.18)
    return jnp.clip(result, -limit, limit).astype(held_as)


def setup_inputs(seed: int = 0) -> dict:
    key_of = jax.random.split(jax.random.key(seed), 14)
    q_heads = draw_q_heads(jax.random.fold_in(key_of[13], 71), 0)
    k_heads = draw_k_heads(jax.random.fold_in(key_of[13], 71), 0)
    v_heads = scatter_about(key_of[2], (TOK_A, KV * HD), 1.0, 6.0, ((0, 8), (1, 4)))
    sink_logits = jnp.clip(1.0 + 4.0 * jax.random.uniform(key_of[3], (HEADS,), jnp.float32) ** block_levels(key_of[3], (HEADS,), ((0, 4),), -0.2, 0.2), 1.0, 5.0)
    out_weight = scatter_about(key_of[4], (HEADS * HD, D), HEADS ** -0.5, 1.5, ((1, 4),))
    tokens_b = scatter_about(key_of[5], (TOK_B, D), 1.0, 6.0, ((0, 8),))
    moe_gain = jnp.clip(1.0 + 0.18 * jax.random.normal(key_of[6], (D,), jnp.float32), 0.1, 1.9)
    router_group = scatter_about(key_of[7], (D, GROUPS), D ** -0.5, 0.125)
    router_expert = scatter_about(key_of[8], (D, EXPERTS), D ** -0.5, 0.125)
    route_expert = draw_route_expert(jax.random.fold_in(key_of[13], 71), 0)
    expert_gate = scatter_about(key_of[10], (EXPERTS, D, FF), D ** -0.5, 0.125, ((0, 8), (2, 4)))
    expert_up = scatter_about(key_of[11], (EXPERTS, D, FF), D ** -0.5, 0.125, ((0, 8), (2, 4)))
    expert_down = scatter_about(key_of[12], (EXPERTS, FF, D), (FF // 16) ** -0.5, 0.75, ((0, 8), (1, 4)))
    return {"q_heads": q_heads, "k_heads": k_heads, "v_heads": v_heads, "sink_logits": sink_logits, "out_weight": out_weight, "tokens_b": tokens_b, "moe_gain": moe_gain, "router_group": router_group, "router_expert": router_expert, "route_expert": route_expert, "expert_gate": expert_gate, "expert_up": expert_up, "expert_down": expert_down}


def banded(values, blocks, span_len):
    shaped = values.reshape(TOK_A, KV, HD)
    padded = jnp.concatenate([jnp.zeros((span_len, KV, HD), shaped.dtype), shaped], axis=0)
    padded = padded.reshape(blocks + 1, span_len, KV, HD)
    band = jnp.concatenate([padded[:-1], padded[1:]], axis=1)
    return jnp.moveaxis(band, 2, 0)

def gate_weights(normed, routes, router_group, router_expert):
    group_logits = jnp.dot(normed, router_group, preferred_element_type=jnp.float32)
    expert_logits = jnp.dot(normed, router_expert, preferred_element_type=jnp.float32)
    group_count = router_group.shape[1]
    expert_count = router_expert.shape[1]
    chosen_group = routes[:, 0] // (expert_count // group_count)
    group_match = chosen_group[:, None] == jnp.arange(group_count, dtype=jnp.int32)[None, :]
    group_share = lax.optimization_barrier(jnp.sum(jnp.where(group_match, jax.nn.softmax(group_logits, axis=-1), 0.0), axis=-1))
    expert_match = routes[:, :, None] == jnp.arange(expert_count, dtype=jnp.int32)[None, None, :]
    picked = lax.optimization_barrier(jnp.sum(jnp.where(expert_match, expert_logits[:, None, :], 0.0), axis=-1))
    return group_share[:, None] * jax.nn.softmax(picked, axis=-1)

def reference(q_heads, k_heads, v_heads, sink_logits, out_weight, tokens_b, moe_gain, router_group, router_expert, route_expert, expert_gate, expert_up, expert_down):
    span_len = WINDOW
    blocks = TOK_A // span_len
    group_size = HEADS // KV
    query_blocks = jnp.moveaxis(q_heads.reshape(blocks, span_len, KV, group_size, HD), 2, 0)
    key_band = banded(k_heads, blocks, span_len)
    value_band = banded(v_heads, blocks, span_len)
    query_index = jnp.arange(span_len, dtype=jnp.int32)[:, None]
    key_index = jnp.arange(2 * span_len, dtype=jnp.int32)[None, :]
    distance = query_index + span_len - key_index
    key_place = jnp.arange(blocks, dtype=jnp.int32)[:, None, None] * span_len + key_index[None] - span_len
    allowed = (distance >= 0)[None] & (distance < span_len)[None] & (key_place >= 0)
    sink_rows = sink_logits.reshape(KV, group_size)

    def one_head(packed):
        query_block, key_rows, value_rows, sink_row = packed
        scores = jnp.einsum('nqgd,nkd->ngqk', query_block.astype(jnp.float32), key_rows.astype(jnp.float32)) * HD ** (-0.5)
        masked = jnp.where(allowed[:, None], scores, -1e+30)
        sink_full = sink_row[None, :, None]
        row_max = jnp.maximum(lax.optimization_barrier(jnp.max(masked, axis=-1)), sink_full)
        weights_exp = jnp.exp(masked - row_max[..., None])
        denominator = lax.optimization_barrier(jnp.sum(weights_exp, axis=-1)) + jnp.exp(sink_full - row_max)
        probs = lax.optimization_barrier((weights_exp / denominator[..., None]).astype(jnp.bfloat16))
        mixed = jnp.einsum('ngqk,nkd->nqgd', probs.astype(jnp.float32), value_rows.astype(jnp.float32))
        return mixed.astype(jnp.bfloat16)
    attended = lax.map(one_head, (query_blocks, key_band, value_band, sink_rows))
    attended = jnp.moveaxis(attended, 0, 2).reshape(TOK_A, HEADS * HD)
    mixer_out = jnp.dot(attended, out_weight, preferred_element_type=jnp.float32).astype(jnp.bfloat16)
    blocks_b = N_EP * N_TP
    values = tokens_b.astype(jnp.float32)
    normed = (values * lax.rsqrt(lax.optimization_barrier(jnp.mean(values * values, axis=-1, keepdims=True)) + 1e-06) * moe_gain).astype(jnp.bfloat16)
    gates = gate_weights(normed, route_expert, router_group, router_expert)
    flat_routes = route_expert.reshape(blocks_b, 2 * ROW_B)
    onehot = (flat_routes[:, :, None] == jnp.arange(EXPERTS, dtype=jnp.int32)[None, None, :]).astype(jnp.int32)
    places = lax.optimization_barrier(jnp.sum(onehot * jnp.cumsum(onehot, axis=1), axis=2)) - 1
    token_ids = (jnp.arange(TOK_B * 2, dtype=jnp.int32) // 2).reshape(blocks_b, 2 * ROW_B)
    block_ids = jnp.broadcast_to(jnp.arange(blocks_b, dtype=jnp.int32)[:, None], (blocks_b, 2 * ROW_B))
    slot_token = jnp.full((EXPERTS, blocks_b, CAP), TOK_B, jnp.int32).at[flat_routes, block_ids, places].set(token_ids)
    slot_gate = jnp.zeros((EXPERTS, blocks_b, CAP), jnp.float32).at[flat_routes, block_ids, places].set(gates.reshape(blocks_b, 2 * ROW_B))
    padded_rows = jnp.concatenate([normed, jnp.zeros((1, D), jnp.bfloat16)], axis=0)
    hidden_block = FF // N_TP

    def one_expert(running, packed):
        token_list, gate_list, w_gate, w_up, w_down = packed
        rows_in = padded_rows[token_list]
        gate_pre = jnp.dot(rows_in, w_gate, preferred_element_type=jnp.float32)
        up_pre = jnp.dot(rows_in, w_up, preferred_element_type=jnp.float32)
        activated = lax.optimization_barrier((jax.nn.silu(gate_pre) * up_pre).astype(jnp.bfloat16))
        pieces = jnp.einsum('ntf,tfd->ntd', activated.reshape(-1, N_TP, hidden_block).astype(jnp.float32), w_down.reshape(N_TP, hidden_block, D).astype(jnp.float32))
        pieces = lax.optimization_barrier(pieces.astype(jnp.bfloat16)).astype(jnp.float32)
        expert_out = lax.optimization_barrier(lax.optimization_barrier(jnp.sum(pieces, axis=1)).astype(jnp.bfloat16)).astype(jnp.float32)
        running = running.at[token_list].add(gate_list[:, None] * expert_out)
        return (running, None)
    running = jnp.zeros((TOK_B + 1, D), jnp.float32)
    running, _ = lax.scan(one_expert, running, (slot_token.reshape(EXPERTS, -1), slot_gate.reshape(EXPERTS, -1), expert_gate, expert_up, expert_down))
    moe_out = running[:TOK_B].astype(jnp.bfloat16)
    return (mixer_out, moe_out)
```

```python
import functools

import jax
import jax.numpy as jnp
from jax import lax
from jax.experimental import pallas as pl
from jax.experimental.pallas import tpu as pltpu
from jax.sharding import PartitionSpec as P

HEADS = 16
KV = 4
HD = 64
WINDOW = 128
LANES = 128


def shifted(value, axis, steps):
    count = lax.axis_size(axis)
    leading, last = (max(0, -steps), min(count, count - steps))
    return lax.ppermute(value, axis, [(source, source + steps) for source in range(leading, last)])


def flipped(value, axis, bits):
    return lax.ppermute(value, axis, [(i, i ^ bits) for i in range(lax.axis_size(axis))])


def dot_f32(a, b, contract):
    return lax.dot_general(a, b, ((contract[:1], contract[1:]), ((), ())), preferred_element_type=jnp.float32)


def attention_kernel(place_ref, q_ref, kt_ref, vt_ref, halo_ref, sink_ref, out_ref, *, kv_local, group_size):
    span = WINDOW
    rows = q_ref.shape[0]
    query_index = lax.broadcasted_iota(jnp.int32, (span, 2 * span), 0)
    key_index = lax.broadcasted_iota(jnp.int32, (span, 2 * span), 1)
    banded = (key_index > query_index) & (key_index <= query_index + span)
    first_banded = banded & ((key_index >= span) | (place_ref[0] > 0))
    half = kv_local * HD
    for block in range(rows // span):
        here = pl.ds(block * span, span)
        allowed = first_banded if block == 0 else banded
        for kv in range(kv_local):
            heads = pl.ds(kv * HD, HD)
            if block == 0:
                k_band = jnp.concatenate([halo_ref[kv * HD : (kv + 1) * HD, :], kt_ref[heads, here]], axis=1)
                v_band = jnp.concatenate(
                    [halo_ref[half + kv * HD : half + (kv + 1) * HD, :], vt_ref[heads, here]], axis=1
                )
            else:
                k_band = kt_ref[heads, pl.ds((block - 1) * span, 2 * span)]
                v_band = vt_ref[heads, pl.ds((block - 1) * span, 2 * span)]
            mixed = []
            for member in range(group_size):
                head = kv * group_size + member
                scores = dot_f32(q_ref[here, pl.ds(head * HD, HD)], k_band, (1, 0)) * HD ** (-0.5)
                masked = jnp.where(allowed, scores, -1e30)
                sink = sink_ref[head]
                row_max = jnp.maximum(jnp.max(masked, axis=1, keepdims=True), sink)
                weights_exp = jnp.exp(masked - row_max)
                denominator = jnp.sum(weights_exp, axis=1, keepdims=True) + jnp.exp(sink - row_max)
                probs = (weights_exp * (1.0 / denominator)).astype(jnp.bfloat16)
                mixed.append(dot_f32(probs, v_band, (1, 1)))
            out_ref[here, pl.ds(kv * group_size * HD, group_size * HD)] = jnp.concatenate(mixed, axis=1).astype(
                jnp.bfloat16
            )


def attend(place, q_heads, k_t, v_t, halo, sink_logits, kv_local, group_size):
    vmem = pl.BlockSpec(memory_space=pltpu.VMEM)
    smem = pl.BlockSpec(memory_space=pltpu.SMEM)
    return pl.pallas_call(
        functools.partial(attention_kernel, kv_local=kv_local, group_size=group_size),
        out_shape=jax.ShapeDtypeStruct(q_heads.shape, jnp.bfloat16),
        in_specs=[smem, vmem, vmem, vmem, vmem, smem],
        out_specs=vmem,
        cost_estimate=pl.CostEstimate(flops=6_000_000_000, bytes_accessed=2_000_000, transcendentals=0),
        name="attend",
    )(place, q_heads, k_t, v_t, halo, sink_logits)


def projection_kernel(place_ref, *refs):
    *pieces, weight_ref, out_ref = refs
    width = pieces[0].shape[1]
    total = None
    for bits, piece in enumerate(pieces):
        rows = pl.ds(pl.multiple_of((place_ref[1] ^ bits) * width, width), width)
        part = dot_f32(piece[...], weight_ref[rows, :], (1, 0))
        total = part if total is None else total + part
    out_ref[...] = total.astype(jnp.bfloat16)


def project(place, pieces, out_weight):
    rows, width = pieces[0].shape
    tile = rows // 4
    return pl.pallas_call(
        projection_kernel,
        grid_spec=pltpu.PrefetchScalarGridSpec(
            num_scalar_prefetch=1,
            grid=(rows // tile,),
            in_specs=[pl.BlockSpec((tile, width), lambda i, s: (i, 0)) for _ in pieces]
            + [pl.BlockSpec(out_weight.shape, lambda i, s: (0, 0))],
            out_specs=pl.BlockSpec((tile, out_weight.shape[1]), lambda i, s: (i, 0)),
        ),
        out_shape=jax.ShapeDtypeStruct((rows, out_weight.shape[1]), jnp.bfloat16),
        cost_estimate=pl.CostEstimate(flops=2_000_000_000, bytes_accessed=4_000_000, transcendentals=0),
        name="project",
    )(place, *pieces, out_weight)


def dispatch_kernel(place_ref, tokens_ref, gain_ref, group_ref, expert_ref, routes_ref, order_ref, *send_refs):
    groups = group_ref.shape[0]
    experts = expert_ref.shape[0]
    size = experts // groups
    rows, width = tokens_ref.shape
    values = tokens_ref[...].astype(jnp.float32)
    scaled = values * lax.rsqrt(jnp.mean(values * values, axis=-1, keepdims=True) + 1e-06) * gain_ref[...]
    normed = scaled.astype(jnp.bfloat16)
    group_logits = dot_f32(group_ref[...], normed, (1, 1))
    expert_logits = dot_f32(expert_ref[...], normed, (1, 1))
    first = routes_ref[0:1, :]
    second = routes_ref[1:2, :]
    group_index = lax.broadcasted_iota(jnp.int32, (groups, rows), 0)
    in_group = (first >= group_index * size) & (first < (group_index + 1) * size)
    group_exp = jnp.exp(group_logits - jnp.max(group_logits, axis=0, keepdims=True))
    share = jnp.sum(jnp.where(in_group, group_exp, 0.0), axis=0, keepdims=True) / jnp.sum(
        group_exp, axis=0, keepdims=True
    )
    expert_index = lax.broadcasted_iota(jnp.int32, (experts, rows), 0)
    pick_first = jnp.sum(jnp.where(expert_index == first, expert_logits, 0.0), axis=0, keepdims=True)
    pick_second = jnp.sum(jnp.where(expert_index == second, expert_logits, 0.0), axis=0, keepdims=True)
    pick_max = jnp.maximum(pick_first, pick_second)
    exp_first = jnp.exp(pick_first - pick_max)
    exp_second = jnp.exp(pick_second - pick_max)
    pick_sum = exp_first + exp_second
    gate_first = share * (exp_first / pick_sum)
    gate_second = share * (exp_second / pick_sum)
    earlier = lax.broadcasted_iota(jnp.int32, (rows, rows), 0) < lax.broadcasted_iota(jnp.int32, (rows, rows), 1)
    member = jnp.where(in_group, 1.0, 0.0)
    rank = dot_f32(member.astype(jnp.bfloat16), jnp.where(earlier, 1.0, 0.0).astype(jnp.bfloat16), (1, 0))
    chunk = (group_index ^ place_ref[2]) * (rows // groups)
    slot = jnp.sum(member * (chunk.astype(jnp.float32) + rank), axis=0, keepdims=True).astype(jnp.int32)
    order = jnp.where(lax.broadcasted_iota(jnp.int32, (rows, rows), 0) == slot, 1.0, 0.0).astype(jnp.bfloat16)
    order_ref[...] = order
    base = jnp.sum(jnp.where(in_group, group_index * size, 0), axis=0, keepdims=True)
    line = lax.broadcasted_iota(jnp.int32, (LANES, rows), 0)
    local = jnp.where(line < size, line, line - size) + base
    gate = jnp.where(local == first, gate_first, 0.0) + jnp.where(local == second, gate_second, 0.0)
    high = gate.astype(jnp.bfloat16).astype(jnp.float32)
    columns = jnp.where(line < size, high, jnp.where(line < 2 * size, gate - high, 0.0)).astype(jnp.bfloat16)
    moved = dot_f32(order, normed, (1, 0)).astype(jnp.bfloat16)
    moved_gates = dot_f32(order, columns, (1, 1)).astype(jnp.bfloat16)
    step = rows // groups
    for k, send in enumerate(send_refs):
        send[:, :width] = moved[k * step : (k + 1) * step]
        send[:, width:] = moved_gates[k * step : (k + 1) * step]


def dispatch(place, tokens, gain, group_t, expert_t, routes_t, rows):
    width = tokens.shape[1]
    groups = group_t.shape[0]
    step = rows // groups
    whole = lambda shape: pl.BlockSpec(shape, lambda i, s: tuple(0 for _ in shape))
    return pl.pallas_call(
        dispatch_kernel,
        grid_spec=pltpu.PrefetchScalarGridSpec(
            num_scalar_prefetch=1,
            grid=(1,),
            in_specs=[
                pl.BlockSpec((rows, width), lambda i, s: (s[1], 0)),
                whole((1, width)),
                whole(group_t.shape),
                whole(expert_t.shape),
                pl.BlockSpec((2, rows), lambda i, s: (0, s[1])),
            ],
            out_specs=[whole((rows, rows))] + [whole((step, width + LANES)) for _ in range(groups)],
        ),
        out_shape=[jax.ShapeDtypeStruct((rows, rows), jnp.bfloat16)]
        + [jax.ShapeDtypeStruct((step, width + LANES), jnp.bfloat16) for _ in range(groups)],
        cost_estimate=pl.CostEstimate(flops=1_000_000_000, bytes_accessed=2_000_000, transcendentals=0),
        name="dispatch",
    )(place, tokens, gain.reshape(1, width), group_t, expert_t, routes_t)


def experts_kernel(place_ref, *refs, sizes, size, tile):
    count = len(sizes)
    pieces = refs[:count]
    gate_ref, up_ref, down_ref, here_ref, there_ref, rows_ref = refs[count:]
    exp_local, width, hidden = gate_ref.shape
    at = 0
    for piece, rows in zip(pieces, sizes):
        rows_ref[at : at + rows, :] = piece[...]
        at += rows
    half = at // 2
    line = lax.broadcasted_iota(jnp.int32, (tile, LANES), 1)
    for start in range(0, at, tile):
        held = rows_ref[start : start + tile, :width]
        gates = rows_ref[start : start + tile, width:].astype(jnp.float32)
        active = []
        for e in range(exp_local):
            own = place_ref[3] * exp_local + e
            gate = jnp.sum(
                jnp.where((line == own) | (line == own + size), gates, 0.0), axis=1, keepdims=True
            )
            gate_pre = dot_f32(held, gate_ref[e], (1, 0))
            up_pre = dot_f32(held, up_ref[e], (1, 0))
            active.append((jax.nn.silu(gate_pre) * up_pre * gate).astype(jnp.bfloat16))
        result = None
        for e in range(exp_local):
            part = dot_f32(active[e], down_ref[e], (1, 0))
            result = part if result is None else result + part
        result = result.astype(jnp.bfloat16)
        if start < half:
            here_ref[start : start + tile, :] = result
        else:
            there_ref[start - half : start - half + tile, :] = result


def run_experts(place, pieces, expert_gate, expert_up, expert_down, size):
    sizes = tuple(piece.shape[0] for piece in pieces)
    rows = sum(sizes)
    width = expert_gate.shape[1]
    vmem = pl.BlockSpec(memory_space=pltpu.VMEM)
    smem = pl.BlockSpec(memory_space=pltpu.SMEM)
    return pl.pallas_call(
        functools.partial(experts_kernel, sizes=sizes, size=size, tile=min(rows // 2, 256)),
        out_shape=[jax.ShapeDtypeStruct((rows // 2, width), jnp.bfloat16) for _ in range(2)],
        in_specs=[smem] + [vmem] * (len(pieces) + 3),
        out_specs=[vmem, vmem],
        scratch_shapes=[pltpu.VMEM((rows, width + LANES), jnp.bfloat16)],
        cost_estimate=pl.CostEstimate(flops=rows * 7_000_000, bytes_accessed=15_000_000, transcendentals=0),
        name="experts",
    )(place, *pieces, expert_gate, expert_up, expert_down)


def combine_kernel(order_ref, *refs):
    *pieces, out_ref = refs
    rows = jnp.concatenate([piece[...] for piece in pieces], axis=0)
    out_ref[...] = dot_f32(order_ref[...], rows, (0, 0)).astype(jnp.bfloat16)


def combine(order, pieces):
    vmem = pl.BlockSpec(memory_space=pltpu.VMEM)
    return pl.pallas_call(
        combine_kernel,
        out_shape=jax.ShapeDtypeStruct((order.shape[0], pieces[0].shape[1]), jnp.bfloat16),
        in_specs=[vmem] * (len(pieces) + 1),
        out_specs=vmem,
        name="combine",
    )(order, *pieces)


def added(*values):
    return functools.reduce(jnp.add, [v.astype(jnp.float32) for v in values]).astype(jnp.bfloat16)


def gather_plane(own, core_bit, side_bit):
    half = own.shape[0] // 2
    across = flipped(own, "tp", side_bit)
    along = flipped(own, "ep", 1)
    far_low = flipped(across[:half], "ep", 1)
    far_high = flipped(along[half:], "tp", side_bit)
    ours = [own, across, along, far_low, far_high]
    return ours + [flipped(piece, "tp", core_bit) for piece in ours]


def reduce_plane(here, there, core_bit, side_bit):
    step = here.shape[0] // 4
    half = step // 2
    other = flipped(there, "tp", core_bit)
    part = lambda low, high: added(here[low:high], other[low:high])
    far_low = flipped(part(3 * step, 3 * step + half), "ep", 1)
    far_high = flipped(part(3 * step + half, 4 * step), "tp", side_bit)
    across_high = flipped(part(step + half, 2 * step), "tp", side_bit)
    along_low = flipped(part(2 * step, 2 * step + half), "ep", 1)
    across_low = flipped(added(here[step : step + half], other[step : step + half], far_low), "tp", side_bit)
    along_high = flipped(
        added(here[2 * step + half : 3 * step], other[2 * step + half : 3 * step], far_high), "ep", 1
    )
    low = added(here[:half], other[:half], across_low, along_low)
    high = added(here[half:step], other[half:step], across_high, along_high)
    return low, high


def per_device(
    q_heads,
    k_heads,
    v_heads,
    sink_logits,
    out_weight,
    tokens_b,
    moe_gain,
    router_group,
    router_expert,
    route_expert,
    expert_gate,
    expert_up,
    expert_down,
):
    tp_count = lax.axis_size("tp")
    ep_count = lax.axis_size("ep")
    groups = router_group.shape[1]
    experts = router_expert.shape[1]
    exp_local = expert_gate.shape[0]
    members = ep_count // groups
    size = experts // groups
    rows_dev = tokens_b.shape[0] // tp_count
    capacity = min(4 * rows_dev // experts, rows_dev // 4)
    by_group = (
        tp_count == 4
        and members == 2
        and groups & (groups - 1) == 0
        and members * exp_local == size
        and rows_dev // groups <= exp_local * capacity
    )
    ep_index = lax.axis_index("ep")
    tp_index = lax.axis_index("tp")
    place = jnp.stack([ep_index, tp_index, ep_index // members, ep_index % members]).astype(jnp.int32)

    kv_local = k_heads.shape[1] // HD
    k_t = k_heads.T
    v_t = v_heads.T
    last = k_heads.shape[0] - WINDOW
    halo = shifted(jnp.concatenate([k_t[:, last:], v_t[:, last:]], axis=0), "ep", 1)

    if not by_group:
        attended = attend(place, q_heads, k_t, v_t, halo, sink_logits, kv_local, HEADS // KV)
        mixed = jnp.dot(
            lax.all_gather(attended, "tp", axis=1, tiled=True), out_weight, preferred_element_type=jnp.float32
        )
        return (
            mixed.astype(jnp.bfloat16),
            moe_by_slot(
                tokens_b, moe_gain, router_group, router_expert, route_expert, expert_gate, expert_up, expert_down
            ),
        )

    core_bit, side_bit = 1, 2
    order, *sends = dispatch(
        place, tokens_b, moe_gain, router_group.T, router_expert.T, route_expert.T, rows_dev
    )
    arrived = [sends[0]] + [flipped(sends[k], "ep", k * members) for k in range(1, groups)]
    attended = attend(place, q_heads, k_t, v_t, halo, sink_logits, kv_local, HEADS // KV)
    pieces = gather_plane(jnp.concatenate(arrived, axis=0), core_bit, side_bit)
    attended_core = flipped(attended, "tp", core_bit)
    attended_side = flipped(attended, "tp", side_bit)
    attended_both = flipped(attended_side, "tp", core_bit)
    here, there = run_experts(place, pieces, expert_gate, expert_up, expert_down, size)
    low, high = reduce_plane(here, there, core_bit, side_bit)
    mixer_out = project(place, [attended, attended_core, attended_side, attended_both], out_weight)
    step = rows_dev // groups
    totals = jnp.split(low, low.shape[0] // step) + jnp.split(high, high.shape[0] // step)
    returned = [totals[0]] + [flipped(totals[k], "ep", k * members) for k in range(1, groups)]
    return (mixer_out, combine(order, returned))


def normalize(rows_in, gain):
    values = rows_in.astype(jnp.float32)
    scaled = values * lax.rsqrt(jnp.mean(values * values, axis=-1, keepdims=True) + 1e-06) * gain
    return scaled.astype(jnp.bfloat16)


def gate_weights(normed, routes, router_group, router_expert):
    group_logits = jnp.dot(normed, router_group, preferred_element_type=jnp.float32)
    expert_logits = jnp.dot(normed, router_expert, preferred_element_type=jnp.float32)
    group_count = router_group.shape[1]
    expert_count = router_expert.shape[1]
    chosen_group = routes[:, 0] // (expert_count // group_count)
    group_match = chosen_group[:, None] == jnp.arange(group_count, dtype=jnp.int32)[None, :]
    group_share = jnp.sum(jnp.where(group_match, jax.nn.softmax(group_logits, axis=-1), 0.0), axis=-1)
    expert_match = routes[:, :, None] == jnp.arange(expert_count, dtype=jnp.int32)[None, None, :]
    picked = jnp.sum(jnp.where(expert_match, expert_logits[:, None, :], 0.0), axis=-1)
    return group_share[:, None] * jax.nn.softmax(picked, axis=-1)


def moe_by_slot(
    tokens_b, moe_gain, router_group, router_expert, route_expert, expert_gate, expert_up, expert_down
):
    tp_count = lax.axis_size("tp")
    tp_index = lax.axis_index("tp")
    exp_local = expert_gate.shape[0]
    expert_count = exp_local * lax.axis_size("ep")
    rows_dev = tokens_b.shape[0] // tp_count
    width = tokens_b.shape[1]
    capacity = min(4 * rows_dev // expert_count, rows_dev // 4)
    routes = lax.dynamic_slice_in_dim(route_expert, tp_index * rows_dev, rows_dev, 0)
    normed = normalize(lax.dynamic_slice_in_dim(tokens_b, tp_index * rows_dev, rows_dev, 0), moe_gain)
    flat_routes = routes.reshape(-1)
    onehot = (flat_routes[:, None] == jnp.arange(expert_count, dtype=jnp.int32)[None, :]).astype(jnp.int32)
    places = jnp.sum(onehot * jnp.cumsum(onehot, axis=0), axis=1) - 1
    target = flat_routes * capacity + places
    buffer = jnp.zeros((expert_count * capacity, width), jnp.bfloat16)
    buffer = buffer.at[target].set(jnp.repeat(normed, 2, axis=0))
    buffer = buffer.reshape(expert_count // exp_local, exp_local, 1, capacity, width)
    delivered = lax.all_to_all(buffer, "ep", split_axis=0, concat_axis=0, tiled=True)
    arrived = lax.all_gather(delivered, "tp", axis=2, tiled=True)
    gates = gate_weights(normed, routes, router_group, router_expert)
    gate_pre = jnp.einsum("setcd,edf->setcf", arrived, expert_gate, preferred_element_type=jnp.float32)
    up_pre = jnp.einsum("setcd,edf->setcf", arrived, expert_up, preferred_element_type=jnp.float32)
    activated = (jax.nn.silu(gate_pre) * up_pre).astype(jnp.bfloat16)
    partial_value = jnp.einsum("setcf,efd->setcd", activated, expert_down, preferred_element_type=jnp.float32)
    summed = lax.psum_scatter(partial_value.astype(jnp.bfloat16), "tp", scatter_dimension=2, tiled=True)
    returned = lax.all_to_all(summed, "ep", split_axis=0, concat_axis=0, tiled=True)
    picked_rows = returned.reshape(expert_count * capacity, width)[target].reshape(rows_dev, 2, width)
    return jnp.sum(gates[:, :, None] * picked_rows.astype(jnp.float32), axis=1).astype(jnp.bfloat16)


def solution(mesh):
    in_specs = (
        P("ep", "tp"),
        P("ep", "tp"),
        P("ep", "tp"),
        P("tp"),
        P(None, "tp"),
        P("ep", None),
        P(),
        P(),
        P(),
        P("ep", None),
        P("ep", None, "tp"),
        P("ep", None, "tp"),
        P("ep", "tp", None),
    )
    out_specs = (P("ep", "tp"), P(("ep", "tp"), None))
    return jax.shard_map(per_device, mesh=mesh, in_specs=in_specs, out_specs=out_specs, check_vma=False)
```

```python
import functools

import jax
import jax.numpy as jnp
from jax import lax
from jax.experimental import pallas as pl
from jax.experimental.pallas import tpu as pltpu
from jax.sharding import PartitionSpec as P


HEADS = 16
KV = 4
HD = 64
WINDOW = 128
LANES = 128


def shifted(value, axis, steps):
    count = lax.axis_size(axis)
    leading, last = (max(0, -steps), min(count, count - steps))
    return lax.ppermute(value, axis, [(source, source + steps) for source in range(leading, last)])


def flipped(value, axis, bits):
    return lax.ppermute(value, axis, [(i, i ^ bits) for i in range(lax.axis_size(axis))])


def in_vmem(*values):
    return [pltpu.with_memory_space_constraint(v, pltpu.VMEM) for v in values]


def in_hbm(*values):
    return [pltpu.with_memory_space_constraint(v, pltpu.HBM) for v in values]


def vmem_out(shape, dtype=jnp.bfloat16):
    return pltpu.VMEM(shape, dtype)


def dot_f32(a, b, contract):
    return lax.dot_general(a, b, ((contract[:1], contract[1:]), ((), ())), preferred_element_type=jnp.float32)


def attention_kernel(place_ref, q_ref, kt_ref, vt_ref, sink_ref, *refs, first, kv_local, group_size):
    *halo, out_ref = refs
    span = WINDOW
    query_index = lax.broadcasted_iota(jnp.int32, (span, 2 * span), 0)
    key_index = lax.broadcasted_iota(jnp.int32, (span, 2 * span), 1)
    banded = (key_index > query_index) & (key_index <= query_index + span)
    half = kv_local * HD
    for block in range(out_ref.shape[0] // span):
        here = pl.ds((first + block) * span, span)
        band = pl.ds((first + block - 1) * span, 2 * span)
        at_start = first + block == 0
        allowed = banded & ((key_index >= span) | (place_ref[0] > 0)) if at_start else banded
        for kv in range(kv_local):
            heads = pl.ds(kv * HD, HD)
            if at_start:
                (halo_ref,) = halo
                k_band = jnp.concatenate([halo_ref[kv * HD : (kv + 1) * HD, :], kt_ref[heads, here]], axis=1)
                v_band = jnp.concatenate(
                    [halo_ref[half + kv * HD : half + (kv + 1) * HD, :], vt_ref[heads, here]], axis=1
                )
            else:
                k_band = kt_ref[heads, band]
                v_band = vt_ref[heads, band]
            mixed = []
            for member in range(group_size):
                head = kv * group_size + member
                scores = dot_f32(q_ref[here, pl.ds(head * HD, HD)], k_band, (1, 0)) * HD ** (-0.5)
                masked = jnp.where(allowed, scores, -1e30)
                sink = sink_ref[head]
                row_max = jnp.maximum(jnp.max(masked, axis=1, keepdims=True), sink)
                weights_exp = jnp.exp(masked - row_max)
                denominator = jnp.sum(weights_exp, axis=1, keepdims=True) + jnp.exp(sink - row_max)
                probs = (weights_exp * (1.0 / denominator)).astype(jnp.bfloat16)
                mixed.append(dot_f32(probs, v_band, (1, 1)))
            out_ref[block * span : (block + 1) * span, pl.ds(kv * group_size * HD, group_size * HD)] = (
                jnp.concatenate(mixed, axis=1).astype(jnp.bfloat16)
            )


def attend(place, q_heads, k_t, v_t, sink_logits, first, last, halo):
    kv_local = k_t.shape[0] // HD
    vmem = pl.BlockSpec(memory_space=pltpu.VMEM)
    smem = pl.BlockSpec(memory_space=pltpu.SMEM)
    return pl.pallas_call(
        functools.partial(attention_kernel, first=first, kv_local=kv_local, group_size=HEADS // KV),
        out_shape=jax.ShapeDtypeStruct(((last - first) * WINDOW, q_heads.shape[1]), jnp.bfloat16),
        in_specs=[smem, vmem, vmem, vmem, smem] + [vmem] * len(halo),
        out_specs=vmem,
        cost_estimate=pl.CostEstimate(flops=3_000_000_000, bytes_accessed=2_000_000, transcendentals=0),
        compiler_params=pltpu.CompilerParams(vmem_limit_bytes=12 << 20),
        name="attend",
    )(place, q_heads, k_t, v_t, sink_logits, *halo)


def projection_kernel(place_ref, *refs, count, first, steps):
    pieces, weight_ref = refs[:count], refs[count]
    out_ref, tile_ref, sems = refs[-3:]
    rows, width = pieces[0].shape
    tile = rows // steps
    copies = []
    for i in range(steps):
        total = None
        for bits, piece in enumerate(pieces):
            lines = pl.ds(pl.multiple_of((place_ref[1] ^ bits) * width, width), width)
            product = dot_f32(piece[i * tile : (i + 1) * tile, :], weight_ref[lines, :], (1, 0))
            total = product if total is None else total + product
        tile_ref[i] = total.astype(jnp.bfloat16)
        copies.append(
            pltpu.make_async_copy(tile_ref.at[i], out_ref.at[pl.ds(first + i * tile, tile), :], sems.at[i])
        )
        copies[-1].start()
    for copy in copies:
        copy.wait()


def project(place, pieces, out_weight, part, parts, held):
    rows = pieces[0].shape[0]
    steps = 2
    vmem = pl.BlockSpec(memory_space=pltpu.VMEM)
    operands = [place, *in_vmem(*pieces, out_weight), *held]
    return pl.pallas_call(
        functools.partial(projection_kernel, count=len(pieces), first=part * rows, steps=steps),
        in_specs=[pl.BlockSpec(memory_space=pltpu.SMEM)]
        + [vmem] * (len(pieces) + 1)
        + [pl.BlockSpec(memory_space=pl.ANY) for _ in held],
        out_specs=pl.BlockSpec(memory_space=pl.ANY),
        out_shape=pltpu.HBM((rows * parts, out_weight.shape[1]), jnp.bfloat16),
        scratch_shapes=[
            pltpu.VMEM((steps, rows // steps, out_weight.shape[1]), jnp.bfloat16),
            pltpu.SemaphoreType.DMA((steps,)),
        ],
        input_output_aliases={len(operands) - 1: 0} if held else {},
        cost_estimate=pl.CostEstimate(flops=1_000_000_000, bytes_accessed=3_000_000, transcendentals=0),
        compiler_params=pltpu.CompilerParams(vmem_limit_bytes=8 << 20),
        name="project",
    )(*operands)


def dispatch_kernel(
    place_ref, tokens_ref, gain_ref, group_ref, expert_ref, routes_ref, k_ref, v_ref, order_ref, tail_ref, *send_refs
):
    tail_ref[...] = jnp.concatenate([k_ref[...], v_ref[...]], axis=0)
    groups = group_ref.shape[0]
    experts = expert_ref.shape[0]
    size = experts // groups
    rows, width = tokens_ref.shape
    values = tokens_ref[...].astype(jnp.float32)
    scaled = values * lax.rsqrt(jnp.mean(values * values, axis=-1, keepdims=True) + 1e-06) * gain_ref[...]
    normed = scaled.astype(jnp.bfloat16)
    group_logits = dot_f32(group_ref[...], normed, (1, 1))
    expert_logits = dot_f32(expert_ref[...], normed, (1, 1))
    first = routes_ref[0:1, :]
    second = routes_ref[1:2, :]
    group_index = lax.broadcasted_iota(jnp.int32, (groups, rows), 0)
    in_group = (first >= group_index * size) & (first < (group_index + 1) * size)
    group_exp = jnp.exp(group_logits - jnp.max(group_logits, axis=0, keepdims=True))
    share = jnp.sum(jnp.where(in_group, group_exp, 0.0), axis=0, keepdims=True) / jnp.sum(
        group_exp, axis=0, keepdims=True
    )
    expert_index = lax.broadcasted_iota(jnp.int32, (experts, rows), 0)
    pick_first = jnp.sum(jnp.where(expert_index == first, expert_logits, 0.0), axis=0, keepdims=True)
    pick_second = jnp.sum(jnp.where(expert_index == second, expert_logits, 0.0), axis=0, keepdims=True)
    pick_max = jnp.maximum(pick_first, pick_second)
    exp_first = jnp.exp(pick_first - pick_max)
    exp_second = jnp.exp(pick_second - pick_max)
    pick_sum = exp_first + exp_second
    gate_first = share * (exp_first / pick_sum)
    gate_second = share * (exp_second / pick_sum)
    earlier = lax.broadcasted_iota(jnp.int32, (rows, rows), 0) < lax.broadcasted_iota(jnp.int32, (rows, rows), 1)
    member = jnp.where(in_group, 1.0, 0.0)
    rank = dot_f32(member.astype(jnp.bfloat16), jnp.where(earlier, 1.0, 0.0).astype(jnp.bfloat16), (1, 0))
    chunk = (group_index ^ place_ref[2]) * (rows // groups)
    slot = jnp.sum(member * (chunk.astype(jnp.float32) + rank), axis=0, keepdims=True).astype(jnp.int32)
    order = jnp.where(lax.broadcasted_iota(jnp.int32, (rows, rows), 0) == slot, 1.0, 0.0).astype(jnp.bfloat16)
    order_ref[...] = order
    base = jnp.sum(jnp.where(in_group, group_index * size, 0), axis=0, keepdims=True)
    line = lax.broadcasted_iota(jnp.int32, (LANES, rows), 0)
    local = jnp.where(line < size, line, line - size) + base
    gate = jnp.where(local == first, gate_first, 0.0) + jnp.where(local == second, gate_second, 0.0)
    high = gate.astype(jnp.bfloat16).astype(jnp.float32)
    columns = jnp.where(line < size, high, jnp.where(line < 2 * size, gate - high, 0.0)).astype(jnp.bfloat16)
    moved = dot_f32(order, normed, (1, 0)).astype(jnp.bfloat16)
    moved_gates = dot_f32(order, columns, (1, 1)).astype(jnp.bfloat16)
    step = rows // groups
    for k, send in enumerate(send_refs):
        send[:, :width] = moved[k * step : (k + 1) * step]
        send[:, width:] = moved_gates[k * step : (k + 1) * step]


def dispatch(place, tokens, gain, group_t, expert_t, routes_t, k_t, v_t, rows):
    width = tokens.shape[1]
    groups = group_t.shape[0]
    step = rows // groups
    last = k_t.shape[1] // WINDOW - 1
    whole = lambda shape: pl.BlockSpec(shape, lambda i, s: tuple(0 for _ in shape))
    return pl.pallas_call(
        dispatch_kernel,
        grid_spec=pltpu.PrefetchScalarGridSpec(
            num_scalar_prefetch=1,
            grid=(1,),
            in_specs=[
                pl.BlockSpec((rows, width), lambda i, s: (s[1], 0)),
                whole((1, width)),
                whole(group_t.shape),
                whole(expert_t.shape),
                pl.BlockSpec((2, rows), lambda i, s: (0, s[1])),
                pl.BlockSpec((k_t.shape[0], WINDOW), lambda i, s: (0, last)),
                pl.BlockSpec((v_t.shape[0], WINDOW), lambda i, s: (0, last)),
            ],
            out_specs=[whole((rows, rows)), whole((k_t.shape[0] + v_t.shape[0], WINDOW))] + [whole((step, width + LANES)) for _ in range(groups)],
        ),
        out_shape=[
            jax.ShapeDtypeStruct((rows, rows), jnp.bfloat16),
            jax.ShapeDtypeStruct((k_t.shape[0] + v_t.shape[0], WINDOW), jnp.bfloat16),
        ]
        + [jax.ShapeDtypeStruct((step, width + LANES), jnp.bfloat16) for _ in range(groups)],
        cost_estimate=pl.CostEstimate(flops=1_000_000_000, bytes_accessed=2_000_000, transcendentals=0),
        compiler_params=pltpu.CompilerParams(vmem_limit_bytes=12 << 20),
        name="dispatch",
    )(place, *in_hbm(tokens, gain.reshape(1, width), group_t, expert_t, routes_t, k_t, v_t))


def experts_kernel(place_ref, *refs, sizes, size):
    count = len(sizes)
    pieces = refs[:count]
    gate_ref, up_ref, down_ref, out_ref, rows_ref = refs[count:]
    exp_local, width, _ = gate_ref.shape
    at = 0
    for piece, rows in zip(pieces, sizes):
        rows_ref[at : at + rows, :] = piece[...]
        at += rows
    held = rows_ref[:, :width]
    gates = rows_ref[:, width:].astype(jnp.float32)
    line = lax.broadcasted_iota(jnp.int32, gates.shape, 1)
    result = None
    for e in range(exp_local):
        own = place_ref[3] * exp_local + e
        gate = jnp.sum(jnp.where((line == own) | (line == own + size), gates, 0.0), axis=1, keepdims=True)
        gate_pre = dot_f32(held, gate_ref[e], (1, 0))
        up_pre = dot_f32(held, up_ref[e], (1, 0))
        active = (jax.nn.silu(gate_pre) * up_pre * gate).astype(jnp.bfloat16)
        part = dot_f32(active, down_ref[e], (1, 0))
        result = part if result is None else result + part
    out_ref[...] = result.astype(jnp.bfloat16)


def run_experts(place, pieces, expert_gate, expert_up, expert_down, size):
    sizes = tuple(piece.shape[0] for piece in pieces)
    rows = sum(sizes)
    width = expert_gate.shape[1]
    vmem = pl.BlockSpec(memory_space=pltpu.VMEM)
    smem = pl.BlockSpec(memory_space=pltpu.SMEM)
    return pl.pallas_call(
        functools.partial(experts_kernel, sizes=sizes, size=size),
        out_shape=vmem_out((rows, width)),
        in_specs=[smem] + [vmem] * (len(pieces) + 3),
        out_specs=vmem,
        scratch_shapes=[pltpu.VMEM((rows, width + LANES), jnp.bfloat16)],
        cost_estimate=pl.CostEstimate(flops=rows * 7_000_000, bytes_accessed=15_000_000, transcendentals=0),
        compiler_params=pltpu.CompilerParams(vmem_limit_bytes=14 << 20),
        name="experts",
    )(place, *in_vmem(*pieces, expert_gate, expert_up, expert_down))


def combine_kernel(order_ref, *refs):
    *pieces, out_ref = refs
    rows = jnp.concatenate([piece[...] for piece in pieces], axis=0)
    out_ref[...] = dot_f32(order_ref[...], rows, (0, 0)).astype(jnp.bfloat16)


def combine(order, pieces):
    vmem = pl.BlockSpec(memory_space=pltpu.VMEM)
    return pl.pallas_call(
        combine_kernel,
        out_shape=jax.ShapeDtypeStruct((order.shape[0], pieces[0].shape[1]), jnp.bfloat16),
        in_specs=[vmem] * (len(pieces) + 1),
        out_specs=vmem,
        compiler_params=pltpu.CompilerParams(vmem_limit_bytes=8 << 20),
        name="combine",
    )(*in_vmem(order, *pieces))


def sums_kernel(*refs, plan):
    values, outs = refs[: len(refs) - len(plan)], refs[len(refs) - len(plan) :]
    for out, segments in zip(outs, plan):
        for at, rows, terms in segments:
            parts = [values[i][start : start + rows, :].astype(jnp.float32) for i, start in terms]
            out[at : at + rows, :] = functools.reduce(jnp.add, parts).astype(jnp.bfloat16)


def sums(plan, *values):
    vmem = pl.BlockSpec(memory_space=pltpu.VMEM)
    width = values[0].shape[1]
    return pl.pallas_call(
        functools.partial(sums_kernel, plan=plan),
        out_shape=[vmem_out((sum(rows for _, rows, _ in segments), width)) for segments in plan],
        in_specs=[vmem] * len(values),
        out_specs=[vmem] * len(plan),
        compiler_params=pltpu.CompilerParams(vmem_limit_bytes=4 << 20),
        name="sums",
    )(*in_vmem(*values))


def gather_plane(own, core_bit, side_bit):
    half = own.shape[0] // 2
    across = flipped(own, "tp", side_bit)
    along = flipped(own, "ep", 1)
    far_low = flipped(across[:half], "ep", 1)
    far_high = flipped(along[half:], "tp", side_bit)
    ours = [own, across, along, far_low, far_high]
    return ours, [flipped(piece, "tp", core_bit) for piece in ours]


def reduce_plane(here, there, core_bit, side_bit, chunks):
    step = here.shape[0] // 4
    half = step // 2
    other = flipped(there, "tp", core_bit)
    both = lambda at: ((0, at), (1, at))
    far_low, far_high = sums(
        (((0, half, both(3 * step)),), ((0, half, both(3 * step + half)),)), here, other
    )
    far_low = flipped(far_low, "ep", 1)
    far_high = flipped(far_high, "tp", side_bit)
    across, along = sums(
        (
            ((0, half, both(step) + ((2, 0),)), (half, half, both(step + half))),
            ((0, half, both(2 * step)), (half, half, both(2 * step + half) + ((3, 0),))),
        ),
        here,
        other,
        far_low,
        far_high,
    )
    across = flipped(across, "tp", side_bit)
    along = flipped(along, "ep", 1)
    piece = step // chunks
    return sums(
        tuple(
            ((0, piece, both(i * piece) + ((2, i * piece), (3, i * piece))),) for i in range(chunks)
        ),
        here,
        other,
        across,
        along,
    )


def per_device(
    q_heads,
    k_heads,
    v_heads,
    sink_logits,
    out_weight,
    tokens_b,
    moe_gain,
    router_group,
    router_expert,
    route_expert,
    expert_gate,
    expert_up,
    expert_down,
):
    tp_count = lax.axis_size("tp")
    ep_count = lax.axis_size("ep")
    groups = router_group.shape[1]
    experts = router_expert.shape[1]
    exp_local = expert_gate.shape[0]
    members = ep_count // groups
    size = experts // groups
    rows_dev = tokens_b.shape[0] // tp_count
    capacity = min(4 * rows_dev // experts, rows_dev // 4)
    by_group = (
        tp_count == 4
        and members == 2
        and groups & (groups - 1) == 0
        and members * exp_local == size
        and rows_dev // groups <= exp_local * capacity
    )
    ep_index = lax.axis_index("ep")
    tp_index = lax.axis_index("tp")
    place = jnp.stack([ep_index, tp_index, ep_index // members, ep_index % members]).astype(jnp.int32)

    k_t = k_heads.T
    v_t = v_heads.T
    blocks = k_heads.shape[0] // WINDOW
    last = k_heads.shape[0] - WINDOW

    if not by_group:
        halo = shifted(jnp.concatenate([k_t[:, last:], v_t[:, last:]], axis=0), "ep", 1)
        attended = attend(place, q_heads, k_t, v_t, sink_logits, 0, blocks, [halo])
        mixed = jnp.dot(
            lax.all_gather(attended, "tp", axis=1, tiled=True), out_weight, preferred_element_type=jnp.float32
        )
        return (
            mixed.astype(jnp.bfloat16),
            moe_by_slot(
                tokens_b, moe_gain, router_group, router_expert, route_expert, expert_gate, expert_up, expert_down
            ),
        )

    core_bit, side_bit = 1, 2
    order, tail, *sends = dispatch(
        place, tokens_b, moe_gain, router_group.T, router_expert.T, route_expert.T, k_t, v_t, rows_dev
    )
    halo = shifted(tail, "ep", 1)
    chunks = ((0, 2), (1, 3)) if groups == 4 else (tuple(range(groups)),)
    arrived = [sends[0]] + [flipped(sends[k], "ep", k * members) for k in range(1, groups)]
    middle = blocks // 2
    attended = []
    for first, end in ((0, middle), (middle, blocks)):
        attended.append(attend(place, q_heads, k_t, v_t, sink_logits, first, end, [halo] if first == 0 else []))
    results = []
    for chunk in chunks:
        own = jnp.concatenate([arrived[k] for k in chunk], axis=0)
        halves = []
        for pieces in gather_plane(own, core_bit, side_bit):
            halves.append(run_experts(place, pieces, expert_gate, expert_up, expert_down, size))
        results.append(halves)
    core = [flipped(part, "tp", core_bit) for part in attended]
    side = [flipped(part, "tp", side_bit) for part in attended]
    cross = [flipped(part, "tp", core_bit) for part in side]
    held = []
    for part in reversed(range(len(attended))):
        pieces = [attended[part], core[part], side[part], cross[part]]
        held = [project(place, pieces, out_weight, part, len(attended), held)]
    (mixer_out,) = held
    returned = {}
    for chunk, (here, there) in zip(chunks, results):
        totals = reduce_plane(here, there, core_bit, side_bit, len(chunk))
        for k, total in zip(chunk, totals):
            returned[k] = flipped(total, "ep", k * members) if k else total
    return (mixer_out, combine(order, [returned[k] for k in range(groups)]))


def normalize(rows_in, gain):
    values = rows_in.astype(jnp.float32)
    scaled = values * lax.rsqrt(jnp.mean(values * values, axis=-1, keepdims=True) + 1e-06) * gain
    return scaled.astype(jnp.bfloat16)


def gate_weights(normed, routes, router_group, router_expert):
    group_logits = jnp.dot(normed, router_group, preferred_element_type=jnp.float32)
    expert_logits = jnp.dot(normed, router_expert, preferred_element_type=jnp.float32)
    group_count = router_group.shape[1]
    expert_count = router_expert.shape[1]
    chosen_group = routes[:, 0] // (expert_count // group_count)
    group_match = chosen_group[:, None] == jnp.arange(group_count, dtype=jnp.int32)[None, :]
    group_share = jnp.sum(jnp.where(group_match, jax.nn.softmax(group_logits, axis=-1), 0.0), axis=-1)
    expert_match = routes[:, :, None] == jnp.arange(expert_count, dtype=jnp.int32)[None, None, :]
    picked = jnp.sum(jnp.where(expert_match, expert_logits[:, None, :], 0.0), axis=-1)
    return group_share[:, None] * jax.nn.softmax(picked, axis=-1)


def moe_by_slot(
    tokens_b, moe_gain, router_group, router_expert, route_expert, expert_gate, expert_up, expert_down
):
    tp_count = lax.axis_size("tp")
    tp_index = lax.axis_index("tp")
    exp_local = expert_gate.shape[0]
    expert_count = exp_local * lax.axis_size("ep")
    rows_dev = tokens_b.shape[0] // tp_count
    width = tokens_b.shape[1]
    capacity = min(4 * rows_dev // expert_count, rows_dev // 4)
    routes = lax.dynamic_slice_in_dim(route_expert, tp_index * rows_dev, rows_dev, 0)
    normed = normalize(lax.dynamic_slice_in_dim(tokens_b, tp_index * rows_dev, rows_dev, 0), moe_gain)
    flat_routes = routes.reshape(-1)
    onehot = (flat_routes[:, None] == jnp.arange(expert_count, dtype=jnp.int32)[None, :]).astype(jnp.int32)
    places = jnp.sum(onehot * jnp.cumsum(onehot, axis=0), axis=1) - 1
    target = flat_routes * capacity + places
    buffer = jnp.zeros((expert_count * capacity, width), jnp.bfloat16)
    buffer = buffer.at[target].set(jnp.repeat(normed, 2, axis=0))
    buffer = buffer.reshape(expert_count // exp_local, exp_local, 1, capacity, width)
    delivered = lax.all_to_all(buffer, "ep", split_axis=0, concat_axis=0, tiled=True)
    arrived = lax.all_gather(delivered, "tp", axis=2, tiled=True)
    gates = gate_weights(normed, routes, router_group, router_expert)
    gate_pre = jnp.einsum("setcd,edf->setcf", arrived, expert_gate, preferred_element_type=jnp.float32)
    up_pre = jnp.einsum("setcd,edf->setcf", arrived, expert_up, preferred_element_type=jnp.float32)
    activated = (jax.nn.silu(gate_pre) * up_pre).astype(jnp.bfloat16)
    partial_value = jnp.einsum("setcf,efd->setcd", activated, expert_down, preferred_element_type=jnp.float32)
    summed = lax.psum_scatter(partial_value.astype(jnp.bfloat16), "tp", scatter_dimension=2, tiled=True)
    returned = lax.all_to_all(summed, "ep", split_axis=0, concat_axis=0, tiled=True)
    picked_rows = returned.reshape(expert_count * capacity, width)[target].reshape(rows_dev, 2, width)
    return jnp.sum(gates[:, :, None] * picked_rows.astype(jnp.float32), axis=1).astype(jnp.bfloat16)


def solution(mesh):
    in_specs = (
        P("ep", "tp"),
        P("ep", "tp"),
        P("ep", "tp"),
        P("tp"),
        P(None, "tp"),
        P("ep", None),
        P(),
        P(),
        P(),
        P("ep", None),
        P("ep", None, "tp"),
        P("ep", None, "tp"),
        P("ep", "tp", None),
    )
    out_specs = (P("ep", "tp"), P(("ep", "tp"), None))

    return jax.shard_map(per_device, mesh=mesh, in_specs=in_specs, out_specs=out_specs, check_vma=False)
```

```python
import functools

import jax
import jax.numpy as jnp
from jax import lax
from jax.experimental import pallas as pl
from jax.experimental.pallas import tpu as pltpu
from jax.sharding import PartitionSpec as P


HEADS = 16
KV = 4
HD = 64
WINDOW = 128
LANES = 128


def shifted(value, axis, steps):
    count = lax.axis_size(axis)
    leading, last = (max(0, -steps), min(count, count - steps))
    return lax.ppermute(value, axis, [(source, source + steps) for source in range(leading, last)])


def flipped(value, axis, bits):
    return lax.ppermute(value, axis, [(i, i ^ bits) for i in range(lax.axis_size(axis))])


def in_vmem(*values):
    return [pltpu.with_memory_space_constraint(v, pltpu.VMEM) for v in values]


def in_hbm(*values):
    return [pltpu.with_memory_space_constraint(v, pltpu.HBM) for v in values]


def vmem_out(shape, dtype=jnp.bfloat16):
    return pltpu.VMEM(shape, dtype)


def dot_f32(a, b, contract):
    return lax.dot_general(a, b, ((contract[:1], contract[1:]), ((), ())), preferred_element_type=jnp.float32)


def attention_kernel(place_ref, q_ref, kt_ref, vt_ref, sink_ref, *refs, first, kv_local, group_size):
    *halo, out_ref = refs
    span = WINDOW
    query_index = lax.broadcasted_iota(jnp.int32, (span, 2 * span), 0)
    key_index = lax.broadcasted_iota(jnp.int32, (span, 2 * span), 1)
    banded = (key_index > query_index) & (key_index <= query_index + span)
    half = kv_local * HD
    for block in range(out_ref.shape[0] // span):
        here = pl.ds((first + block) * span, span)
        band = pl.ds((first + block - 1) * span, 2 * span)
        at_start = first + block == 0
        allowed = banded & ((key_index >= span) | (place_ref[0] > 0)) if at_start else banded
        for kv in range(kv_local):
            heads = pl.ds(kv * HD, HD)
            if at_start:
                (halo_ref,) = halo
                k_band = jnp.concatenate([halo_ref[kv * HD : (kv + 1) * HD, :], kt_ref[heads, here]], axis=1)
                v_band = jnp.concatenate(
                    [halo_ref[half + kv * HD : half + (kv + 1) * HD, :], vt_ref[heads, here]], axis=1
                )
            else:
                k_band = kt_ref[heads, band]
                v_band = vt_ref[heads, band]
            mixed = []
            for member in range(group_size):
                head = kv * group_size + member
                scores = dot_f32(q_ref[here, pl.ds(head * HD, HD)], k_band, (1, 0)) * HD ** (-0.5)
                masked = jnp.where(allowed, scores, -1e30)
                sink = sink_ref[head]
                row_max = jnp.maximum(jnp.max(masked, axis=1, keepdims=True), sink)
                weights_exp = jnp.exp(masked - row_max)
                denominator = jnp.sum(weights_exp, axis=1, keepdims=True) + jnp.exp(sink - row_max)
                probs = (weights_exp * (1.0 / denominator)).astype(jnp.bfloat16)
                mixed.append(dot_f32(probs, v_band, (1, 1)))
            out_ref[block * span : (block + 1) * span, pl.ds(kv * group_size * HD, group_size * HD)] = (
                jnp.concatenate(mixed, axis=1).astype(jnp.bfloat16)
            )


def attend(place, q_heads, k_t, v_t, sink_logits, first, last, halo):
    kv_local = k_t.shape[0] // HD
    vmem = pl.BlockSpec(memory_space=pltpu.VMEM)
    smem = pl.BlockSpec(memory_space=pltpu.SMEM)
    return pl.pallas_call(
        functools.partial(attention_kernel, first=first, kv_local=kv_local, group_size=HEADS // KV),
        out_shape=jax.ShapeDtypeStruct(((last - first) * WINDOW, q_heads.shape[1]), jnp.bfloat16),
        in_specs=[smem, vmem, vmem, vmem, smem] + [vmem] * len(halo),
        out_specs=vmem,
        cost_estimate=pl.CostEstimate(flops=3_000_000_000, bytes_accessed=2_000_000, transcendentals=0),
        compiler_params=pltpu.CompilerParams(vmem_limit_bytes=12 << 20),
        name="attend",
    )(place, q_heads, k_t, v_t, sink_logits, *halo)


def projection_kernel(place_ref, *refs, count, first, steps):
    pieces, weight_ref = refs[:count], refs[count]
    out_ref, tile_ref, sems = refs[-3:]
    rows, width = pieces[0].shape
    tile = rows // steps
    copies = []
    for i in range(steps):
        total = None
        for bits, piece in enumerate(pieces):
            lines = pl.ds(pl.multiple_of((place_ref[1] ^ bits) * width, width), width)
            product = dot_f32(piece[i * tile : (i + 1) * tile, :], weight_ref[lines, :], (1, 0))
            total = product if total is None else total + product
        tile_ref[i] = total.astype(jnp.bfloat16)
        copies.append(
            pltpu.make_async_copy(tile_ref.at[i], out_ref.at[pl.ds(first + i * tile, tile), :], sems.at[i])
        )
        copies[-1].start()
    for copy in copies:
        copy.wait()


def project(place, pieces, out_weight, part, parts, held):
    rows = pieces[0].shape[0]
    steps = 2
    vmem = pl.BlockSpec(memory_space=pltpu.VMEM)
    operands = [place, *in_vmem(*pieces, out_weight), *held]
    return pl.pallas_call(
        functools.partial(projection_kernel, count=len(pieces), first=part * rows, steps=steps),
        in_specs=[pl.BlockSpec(memory_space=pltpu.SMEM)]
        + [vmem] * (len(pieces) + 1)
        + [pl.BlockSpec(memory_space=pl.ANY) for _ in held],
        out_specs=pl.BlockSpec(memory_space=pl.ANY),
        out_shape=pltpu.HBM((rows * parts, out_weight.shape[1]), jnp.bfloat16),
        scratch_shapes=[
            pltpu.VMEM((steps, rows // steps, out_weight.shape[1]), jnp.bfloat16),
            pltpu.SemaphoreType.DMA((steps,)),
        ],
        input_output_aliases={len(operands) - 1: 0} if held else {},
        cost_estimate=pl.CostEstimate(flops=1_000_000_000, bytes_accessed=3_000_000, transcendentals=0),
        compiler_params=pltpu.CompilerParams(vmem_limit_bytes=8 << 20),
        name="project",
    )(*operands)


def dispatch_kernel(
    place_ref, tokens_ref, gain_ref, group_ref, expert_ref, routes_ref, k_ref, v_ref, order_ref, tail_ref, *send_refs
):
    tail_ref[...] = jnp.concatenate([k_ref[...], v_ref[...]], axis=0)
    groups = group_ref.shape[0]
    experts = expert_ref.shape[0]
    size = experts // groups
    rows, width = tokens_ref.shape
    values = tokens_ref[...].astype(jnp.float32)
    scaled = values * lax.rsqrt(jnp.mean(values * values, axis=-1, keepdims=True) + 1e-06) * gain_ref[...]
    normed = scaled.astype(jnp.bfloat16)
    group_logits = dot_f32(group_ref[...], normed, (1, 1))
    expert_logits = dot_f32(expert_ref[...], normed, (1, 1))
    first = routes_ref[0:1, :]
    second = routes_ref[1:2, :]
    group_index = lax.broadcasted_iota(jnp.int32, (groups, rows), 0)
    in_group = (first >= group_index * size) & (first < (group_index + 1) * size)
    group_exp = jnp.exp(group_logits - jnp.max(group_logits, axis=0, keepdims=True))
    share = jnp.sum(jnp.where(in_group, group_exp, 0.0), axis=0, keepdims=True) / jnp.sum(
        group_exp, axis=0, keepdims=True
    )
    expert_index = lax.broadcasted_iota(jnp.int32, (experts, rows), 0)
    pick_first = jnp.sum(jnp.where(expert_index == first, expert_logits, 0.0), axis=0, keepdims=True)
    pick_second = jnp.sum(jnp.where(expert_index == second, expert_logits, 0.0), axis=0, keepdims=True)
    pick_max = jnp.maximum(pick_first, pick_second)
    exp_first = jnp.exp(pick_first - pick_max)
    exp_second = jnp.exp(pick_second - pick_max)
    pick_sum = exp_first + exp_second
    gate_first = share * (exp_first / pick_sum)
    gate_second = share * (exp_second / pick_sum)
    earlier = lax.broadcasted_iota(jnp.int32, (rows, rows), 0) < lax.broadcasted_iota(jnp.int32, (rows, rows), 1)
    member = jnp.where(in_group, 1.0, 0.0)
    rank = dot_f32(member.astype(jnp.bfloat16), jnp.where(earlier, 1.0, 0.0).astype(jnp.bfloat16), (1, 0))
    chunk = (group_index ^ place_ref[2]) * (rows // groups)
    slot = jnp.sum(member * (chunk.astype(jnp.float32) + rank), axis=0, keepdims=True).astype(jnp.int32)
    order = jnp.where(lax.broadcasted_iota(jnp.int32, (rows, rows), 0) == slot, 1.0, 0.0).astype(jnp.bfloat16)
    order_ref[...] = order
    base = jnp.sum(jnp.where(in_group, group_index * size, 0), axis=0, keepdims=True)
    line = lax.broadcasted_iota(jnp.int32, (LANES, rows), 0)
    local = jnp.where(line < size, line, line - size) + base
    gate = jnp.where(local == first, gate_first, 0.0) + jnp.where(local == second, gate_second, 0.0)
    high = gate.astype(jnp.bfloat16).astype(jnp.float32)
    columns = jnp.where(line < size, high, jnp.where(line < 2 * size, gate - high, 0.0)).astype(jnp.bfloat16)
    moved = dot_f32(order, normed, (1, 0)).astype(jnp.bfloat16)
    moved_gates = dot_f32(order, columns, (1, 1)).astype(jnp.bfloat16)
    step = rows // groups
    for k, send in enumerate(send_refs):
        send[:, :width] = moved[k * step : (k + 1) * step]
        send[:, width:] = moved_gates[k * step : (k + 1) * step]


def dispatch(place, tokens, gain, group_t, expert_t, routes_t, k_t, v_t, rows):
    width = tokens.shape[1]
    groups = group_t.shape[0]
    step = rows // groups
    last = k_t.shape[1] // WINDOW - 1
    whole = lambda shape: pl.BlockSpec(shape, lambda i, s: tuple(0 for _ in shape))
    return pl.pallas_call(
        dispatch_kernel,
        grid_spec=pltpu.PrefetchScalarGridSpec(
            num_scalar_prefetch=1,
            grid=(1,),
            in_specs=[
                pl.BlockSpec((rows, width), lambda i, s: (s[1], 0)),
                whole((1, width)),
                whole(group_t.shape),
                whole(expert_t.shape),
                pl.BlockSpec((2, rows), lambda i, s: (0, s[1])),
                pl.BlockSpec((k_t.shape[0], WINDOW), lambda i, s: (0, last)),
                pl.BlockSpec((v_t.shape[0], WINDOW), lambda i, s: (0, last)),
            ],
            out_specs=[whole((rows, rows)), whole((k_t.shape[0] + v_t.shape[0], WINDOW))] + [whole((step, width + LANES)) for _ in range(groups)],
        ),
        out_shape=[
            jax.ShapeDtypeStruct((rows, rows), jnp.bfloat16),
            jax.ShapeDtypeStruct((k_t.shape[0] + v_t.shape[0], WINDOW), jnp.bfloat16),
        ]
        + [jax.ShapeDtypeStruct((step, width + LANES), jnp.bfloat16) for _ in range(groups)],
        cost_estimate=pl.CostEstimate(flops=1_000_000_000, bytes_accessed=2_000_000, transcendentals=0),
        compiler_params=pltpu.CompilerParams(vmem_limit_bytes=12 << 20),
        name="dispatch",
    )(place, *in_hbm(tokens, gain.reshape(1, width), group_t, expert_t, routes_t, k_t, v_t))


def experts_kernel(place_ref, *refs, sizes, size):
    count = len(sizes)
    pieces = refs[:count]
    gate_ref, up_ref, down_ref, out_ref, rows_ref = refs[count:]
    exp_local, width, _ = gate_ref.shape
    at = 0
    for piece, rows in zip(pieces, sizes):
        rows_ref[at : at + rows, :] = piece[...]
        at += rows
    held = rows_ref[:, :width]
    gates = rows_ref[:, width:].astype(jnp.float32)
    line = lax.broadcasted_iota(jnp.int32, gates.shape, 1)
    result = None
    for e in range(exp_local):
        own = place_ref[3] * exp_local + e
        gate = jnp.sum(jnp.where((line == own) | (line == own + size), gates, 0.0), axis=1, keepdims=True)
        gate_pre = dot_f32(held, gate_ref[e], (1, 0))
        up_pre = dot_f32(held, up_ref[e], (1, 0))
        active = (jax.nn.silu(gate_pre) * up_pre * gate).astype(jnp.bfloat16)
        part = dot_f32(active, down_ref[e], (1, 0))
        result = part if result is None else result + part
    out_ref[...] = result.astype(jnp.bfloat16)


def run_experts(place, pieces, expert_gate, expert_up, expert_down, size):
    sizes = tuple(piece.shape[0] for piece in pieces)
    rows = sum(sizes)
    width = expert_gate.shape[1]
    vmem = pl.BlockSpec(memory_space=pltpu.VMEM)
    smem = pl.BlockSpec(memory_space=pltpu.SMEM)
    return pl.pallas_call(
        functools.partial(experts_kernel, sizes=sizes, size=size),
        out_shape=vmem_out((rows, width)),
        in_specs=[smem] + [vmem] * (len(pieces) + 3),
        out_specs=vmem,
        scratch_shapes=[pltpu.VMEM((rows, width + LANES), jnp.bfloat16)],
        cost_estimate=pl.CostEstimate(flops=rows * 7_000_000, bytes_accessed=15_000_000, transcendentals=0),
        compiler_params=pltpu.CompilerParams(vmem_limit_bytes=14 << 20),
        name="experts",
    )(place, *in_vmem(*pieces, expert_gate, expert_up, expert_down))


def combine_kernel(order_ref, *refs, steps):
    *pieces, out_ref, tile_ref, sems = refs
    rows = jnp.concatenate([piece[...] for piece in pieces], axis=0)
    width = rows.shape[1] // steps
    copies = []
    for i in range(steps):
        tile_ref[i] = dot_f32(order_ref[...], rows[:, i * width : (i + 1) * width], (0, 0)).astype(jnp.bfloat16)
        copies.append(
            pltpu.make_async_copy(tile_ref.at[i], out_ref.at[:, pl.ds(i * width, width)], sems.at[i])
        )
        copies[-1].start()
    for copy in copies:
        copy.wait()


def combine(order, pieces):
    vmem = pl.BlockSpec(memory_space=pltpu.VMEM)
    rows, width, steps = order.shape[0], pieces[0].shape[1], 4
    return pl.pallas_call(
        functools.partial(combine_kernel, steps=steps),
        out_shape=pltpu.HBM((rows, width), jnp.bfloat16),
        in_specs=[vmem] * (len(pieces) + 1),
        out_specs=pl.BlockSpec(memory_space=pl.ANY),
        scratch_shapes=[
            pltpu.VMEM((steps, rows, width // steps), jnp.bfloat16),
            pltpu.SemaphoreType.DMA((steps,)),
        ],
        compiler_params=pltpu.CompilerParams(vmem_limit_bytes=8 << 20),
        name="combine",
    )(*in_vmem(order, *pieces))


def sums_kernel(*refs, plan):
    values, outs = refs[: len(refs) - len(plan)], refs[len(refs) - len(plan) :]
    for out, segments in zip(outs, plan):
        for at, rows, terms in segments:
            parts = [values[i][start : start + rows, :].astype(jnp.float32) for i, start in terms]
            out[at : at + rows, :] = functools.reduce(jnp.add, parts).astype(jnp.bfloat16)


def sums(plan, *values):
    vmem = pl.BlockSpec(memory_space=pltpu.VMEM)
    width = values[0].shape[1]
    return pl.pallas_call(
        functools.partial(sums_kernel, plan=plan),
        out_shape=[vmem_out((sum(rows for _, rows, _ in segments), width)) for segments in plan],
        in_specs=[vmem] * len(values),
        out_specs=[vmem] * len(plan),
        compiler_params=pltpu.CompilerParams(vmem_limit_bytes=4 << 20),
        name="sums",
    )(*in_vmem(*values))


def gather_plane(own, core_bit, side_bit):
    half = own.shape[0] // 2
    across = flipped(own, "tp", side_bit)
    along = flipped(own, "ep", 1)
    far_low = flipped(across[:half], "ep", 1)
    far_high = flipped(along[half:], "tp", side_bit)
    ours = [own, across, along, far_low, far_high]
    return ours, [flipped(piece, "tp", core_bit) for piece in ours]


def reduce_plane(here, there, core_bit, side_bit, chunks):
    step = here.shape[0] // 4
    half = step // 2
    other = flipped(there, "tp", core_bit)
    both = lambda at: ((0, at), (1, at))
    first_side, first_along = sums(
        (
            ((0, half, both(3 * step + half)), (half, half, both(step + half))),
            ((0, half, both(3 * step)), (half, half, both(2 * step))),
        ),
        here,
        other,
    )
    first_side = flipped(first_side, "tp", side_bit)
    first_along = flipped(first_along, "ep", 1)
    second_side, second_along = sums(
        (((0, half, both(step) + ((2, 0),)),), ((0, half, both(2 * step + half) + ((3, 0),)),)),
        here,
        other,
        first_along,
        first_side,
    )
    second_side = flipped(second_side, "tp", side_bit)
    second_along = flipped(second_along, "ep", 1)
    piece = step // chunks
    plan = []
    for at in range(0, step, piece):
        if at < half:
            far = ((2, at), (5, half + at))
        else:
            far = ((4, at), (3, at - half))
        plan.append(((0, piece, both(at) + far),))
    return sums(tuple(plan), here, other, second_side, second_along, first_side, first_along)


def per_device(
    q_heads,
    k_heads,
    v_heads,
    sink_logits,
    out_weight,
    tokens_b,
    moe_gain,
    router_group,
    router_expert,
    route_expert,
    expert_gate,
    expert_up,
    expert_down,
):
    tp_count = lax.axis_size("tp")
    ep_count = lax.axis_size("ep")
    groups = router_group.shape[1]
    experts = router_expert.shape[1]
    exp_local = expert_gate.shape[0]
    members = ep_count // groups
    size = experts // groups
    rows_dev = tokens_b.shape[0] // tp_count
    capacity = min(4 * rows_dev // experts, rows_dev // 4)
    by_group = (
        tp_count == 4
        and members == 2
        and groups & (groups - 1) == 0
        and members * exp_local == size
        and rows_dev // groups <= exp_local * capacity
    )
    ep_index = lax.axis_index("ep")
    tp_index = lax.axis_index("tp")
    place = jnp.stack([ep_index, tp_index, ep_index // members, ep_index % members]).astype(jnp.int32)

    k_t = k_heads.T
    v_t = v_heads.T
    blocks = k_heads.shape[0] // WINDOW
    last = k_heads.shape[0] - WINDOW

    if not by_group:
        halo = shifted(jnp.concatenate([k_t[:, last:], v_t[:, last:]], axis=0), "ep", 1)
        attended = attend(place, q_heads, k_t, v_t, sink_logits, 0, blocks, [halo])
        mixed = jnp.dot(
            lax.all_gather(attended, "tp", axis=1, tiled=True), out_weight, preferred_element_type=jnp.float32
        )
        return (
            mixed.astype(jnp.bfloat16),
            moe_by_slot(
                tokens_b, moe_gain, router_group, router_expert, route_expert, expert_gate, expert_up, expert_down
            ),
        )

    core_bit, side_bit = 1, 2
    order, tail, *sends = dispatch(
        place, tokens_b, moe_gain, router_group.T, router_expert.T, route_expert.T, k_t, v_t, rows_dev
    )
    halo = shifted(tail, "ep", 1)
    chunks = ((0, 2), (1, 3)) if groups == 4 else (tuple(range(groups)),)
    arrived = [sends[0]] + [flipped(sends[k], "ep", k * members) for k in range(1, groups)]
    middle = blocks // 2
    attended = []
    for first, end in ((0, middle), (middle, blocks)):
        attended.append(attend(place, q_heads, k_t, v_t, sink_logits, first, end, [halo] if first == 0 else []))
    results = []
    for chunk in chunks:
        own = jnp.concatenate([arrived[k] for k in chunk], axis=0)
        halves = []
        for pieces in gather_plane(own, core_bit, side_bit):
            halves.append(run_experts(place, pieces, expert_gate, expert_up, expert_down, size))
        results.append(halves)
    core = [flipped(part, "tp", core_bit) for part in attended]
    side = [flipped(part, "tp", side_bit) for part in attended]
    cross = [flipped(part, "tp", core_bit) for part in side]
    held = []
    for part in reversed(range(len(attended))):
        pieces = [attended[part], core[part], side[part], cross[part]]
        held = [project(place, pieces, out_weight, part, len(attended), held)]
    (mixer_out,) = held
    returned = {}
    for chunk, (here, there) in zip(chunks, results):
        totals = reduce_plane(here, there, core_bit, side_bit, len(chunk))
        for k, total in zip(chunk, totals):
            returned[k] = flipped(total, "ep", k * members) if k else total
    moe_out = combine(order, [returned[k] for k in range(groups)])
    return (mixer_out, moe_out)


def normalize(rows_in, gain):
    values = rows_in.astype(jnp.float32)
    scaled = values * lax.rsqrt(jnp.mean(values * values, axis=-1, keepdims=True) + 1e-06) * gain
    return scaled.astype(jnp.bfloat16)


def gate_weights(normed, routes, router_group, router_expert):
    group_logits = jnp.dot(normed, router_group, preferred_element_type=jnp.float32)
    expert_logits = jnp.dot(normed, router_expert, preferred_element_type=jnp.float32)
    group_count = router_group.shape[1]
    expert_count = router_expert.shape[1]
    chosen_group = routes[:, 0] // (expert_count // group_count)
    group_match = chosen_group[:, None] == jnp.arange(group_count, dtype=jnp.int32)[None, :]
    group_share = jnp.sum(jnp.where(group_match, jax.nn.softmax(group_logits, axis=-1), 0.0), axis=-1)
    expert_match = routes[:, :, None] == jnp.arange(expert_count, dtype=jnp.int32)[None, None, :]
    picked = jnp.sum(jnp.where(expert_match, expert_logits[:, None, :], 0.0), axis=-1)
    return group_share[:, None] * jax.nn.softmax(picked, axis=-1)


def moe_by_slot(
    tokens_b, moe_gain, router_group, router_expert, route_expert, expert_gate, expert_up, expert_down
):
    tp_count = lax.axis_size("tp")
    tp_index = lax.axis_index("tp")
    exp_local = expert_gate.shape[0]
    expert_count = exp_local * lax.axis_size("ep")
    rows_dev = tokens_b.shape[0] // tp_count
    width = tokens_b.shape[1]
    capacity = min(4 * rows_dev // expert_count, rows_dev // 4)
    routes = lax.dynamic_slice_in_dim(route_expert, tp_index * rows_dev, rows_dev, 0)
    normed = normalize(lax.dynamic_slice_in_dim(tokens_b, tp_index * rows_dev, rows_dev, 0), moe_gain)
    flat_routes = routes.reshape(-1)
    onehot = (flat_routes[:, None] == jnp.arange(expert_count, dtype=jnp.int32)[None, :]).astype(jnp.int32)
    places = jnp.sum(onehot * jnp.cumsum(onehot, axis=0), axis=1) - 1
    target = flat_routes * capacity + places
    buffer = jnp.zeros((expert_count * capacity, width), jnp.bfloat16)
    buffer = buffer.at[target].set(jnp.repeat(normed, 2, axis=0))
    buffer = buffer.reshape(expert_count // exp_local, exp_local, 1, capacity, width)
    delivered = lax.all_to_all(buffer, "ep", split_axis=0, concat_axis=0, tiled=True)
    arrived = lax.all_gather(delivered, "tp", axis=2, tiled=True)
    gates = gate_weights(normed, routes, router_group, router_expert)
    gate_pre = jnp.einsum("setcd,edf->setcf", arrived, expert_gate, preferred_element_type=jnp.float32)
    up_pre = jnp.einsum("setcd,edf->setcf", arrived, expert_up, preferred_element_type=jnp.float32)
    activated = (jax.nn.silu(gate_pre) * up_pre).astype(jnp.bfloat16)
    partial_value = jnp.einsum("setcf,efd->setcd", activated, expert_down, preferred_element_type=jnp.float32)
    summed = lax.psum_scatter(partial_value.astype(jnp.bfloat16), "tp", scatter_dimension=2, tiled=True)
    returned = lax.all_to_all(summed, "ep", split_axis=0, concat_axis=0, tiled=True)
    picked_rows = returned.reshape(expert_count * capacity, width)[target].reshape(rows_dev, 2, width)
    return jnp.sum(gates[:, :, None] * picked_rows.astype(jnp.float32), axis=1).astype(jnp.bfloat16)


def solution(mesh):
    in_specs = (
        P("ep", "tp"),
        P("ep", "tp"),
        P("ep", "tp"),
        P("tp"),
        P(None, "tp"),
        P("ep", None),
        P(),
        P(),
        P(),
        P("ep", None),
        P("ep", None, "tp"),
        P("ep", None, "tp"),
        P("ep", "tp", None),
    )
    out_specs = (P("ep", "tp"), P(("ep", "tp"), None))

    return jax.shard_map(per_device, mesh=mesh, in_specs=in_specs, out_specs=out_specs, check_vma=False)
```

```python
import functools

import jax
import jax.numpy as jnp
from jax import lax
from jax.experimental import pallas as pl
from jax.experimental.pallas import tpu as pltpu
from jax.sharding import PartitionSpec as P


HEADS = 16
KV = 4
HD = 64
WINDOW = 128
LANES = 128


def shifted(value, axis, steps):
    count = lax.axis_size(axis)
    leading, last = (max(0, -steps), min(count, count - steps))
    return lax.ppermute(value, axis, [(source, source + steps) for source in range(leading, last)])


def flipped(value, axis, bits):
    return lax.ppermute(value, axis, [(i, i ^ bits) for i in range(lax.axis_size(axis))])


def in_vmem(*values):
    return [pltpu.with_memory_space_constraint(v, pltpu.VMEM) for v in values]


def in_hbm(*values):
    return [pltpu.with_memory_space_constraint(v, pltpu.HBM) for v in values]


def vmem_out(shape, dtype=jnp.bfloat16):
    return pltpu.VMEM(shape, dtype)


def dot_f32(a, b, contract):
    return lax.dot_general(a, b, ((contract[:1], contract[1:]), ((), ())), preferred_element_type=jnp.float32)


def attention_kernel(place_ref, q_ref, kt_ref, vt_ref, sink_ref, *refs, first, kv_local, group_size):
    *halo, out_ref = refs
    span = WINDOW
    query_index = lax.broadcasted_iota(jnp.int32, (span, 2 * span), 0)
    key_index = lax.broadcasted_iota(jnp.int32, (span, 2 * span), 1)
    banded = (key_index > query_index) & (key_index <= query_index + span)
    half = kv_local * HD
    for block in range(out_ref.shape[0] // span):
        here = pl.ds((first + block) * span, span)
        band = pl.ds((first + block - 1) * span, 2 * span)
        at_start = first + block == 0
        allowed = banded & ((key_index >= span) | (place_ref[0] > 0)) if at_start else banded
        for kv in range(kv_local):
            heads = pl.ds(kv * HD, HD)
            if at_start:
                (halo_ref,) = halo
                k_band = jnp.concatenate([halo_ref[kv * HD : (kv + 1) * HD, :], kt_ref[heads, here]], axis=1)
                v_band = jnp.concatenate(
                    [halo_ref[half + kv * HD : half + (kv + 1) * HD, :], vt_ref[heads, here]], axis=1
                )
            else:
                k_band = kt_ref[heads, band]
                v_band = vt_ref[heads, band]
            mixed = []
            for member in range(group_size):
                head = kv * group_size + member
                scores = dot_f32(q_ref[here, pl.ds(head * HD, HD)], k_band, (1, 0)) * HD ** (-0.5)
                masked = jnp.where(allowed, scores, -1e30)
                sink = sink_ref[head]
                row_max = jnp.maximum(jnp.max(masked, axis=1, keepdims=True), sink)
                weights_exp = jnp.exp(masked - row_max)
                denominator = jnp.sum(weights_exp, axis=1, keepdims=True) + jnp.exp(sink - row_max)
                probs = (weights_exp * (1.0 / denominator)).astype(jnp.bfloat16)
                mixed.append(dot_f32(probs, v_band, (1, 1)))
            out_ref[block * span : (block + 1) * span, pl.ds(kv * group_size * HD, group_size * HD)] = (
                jnp.concatenate(mixed, axis=1).astype(jnp.bfloat16)
            )


def attend(place, q_heads, k_t, v_t, sink_logits, first, last, halo):
    kv_local = k_t.shape[0] // HD
    vmem = pl.BlockSpec(memory_space=pltpu.VMEM)
    smem = pl.BlockSpec(memory_space=pltpu.SMEM)
    return pl.pallas_call(
        functools.partial(attention_kernel, first=first, kv_local=kv_local, group_size=HEADS // KV),
        out_shape=jax.ShapeDtypeStruct(((last - first) * WINDOW, q_heads.shape[1]), jnp.bfloat16),
        in_specs=[smem, vmem, vmem, vmem, smem] + [vmem] * len(halo),
        out_specs=vmem,
        cost_estimate=pl.CostEstimate(flops=3_000_000_000, bytes_accessed=2_000_000, transcendentals=0),
        compiler_params=pltpu.CompilerParams(vmem_limit_bytes=12 << 20),
        name="attend",
    )(place, q_heads, k_t, v_t, sink_logits, *halo)


def projection_kernel(place_ref, *refs, count, first, steps):
    pieces, weight_ref = refs[:count], refs[count]
    out_ref, tile_ref, sems = refs[-3:]
    rows, width = pieces[0].shape
    tile = rows // steps
    copies = []
    for i in range(steps):
        total = None
        for bits, piece in enumerate(pieces):
            lines = pl.ds(pl.multiple_of((place_ref[1] ^ bits) * width, width), width)
            product = dot_f32(piece[i * tile : (i + 1) * tile, :], weight_ref[lines, :], (1, 0))
            total = product if total is None else total + product
        tile_ref[i] = total.astype(jnp.bfloat16)
        copies.append(
            pltpu.make_async_copy(tile_ref.at[i], out_ref.at[pl.ds(first + i * tile, tile), :], sems.at[i])
        )
        copies[-1].start()
    for copy in copies:
        copy.wait()


def project(place, pieces, out_weight, part, parts, held):
    rows = pieces[0].shape[0]
    steps = 2
    vmem = pl.BlockSpec(memory_space=pltpu.VMEM)
    operands = [place, *in_vmem(*pieces, out_weight), *held]
    return pl.pallas_call(
        functools.partial(projection_kernel, count=len(pieces), first=part * rows, steps=steps),
        in_specs=[pl.BlockSpec(memory_space=pltpu.SMEM)]
        + [vmem] * (len(pieces) + 1)
        + [pl.BlockSpec(memory_space=pl.ANY) for _ in held],
        out_specs=pl.BlockSpec(memory_space=pl.ANY),
        out_shape=pltpu.HBM((rows * parts, out_weight.shape[1]), jnp.bfloat16),
        scratch_shapes=[
            pltpu.VMEM((steps, rows // steps, out_weight.shape[1]), jnp.bfloat16),
            pltpu.SemaphoreType.DMA((steps,)),
        ],
        input_output_aliases={len(operands) - 1: 0} if held else {},
        cost_estimate=pl.CostEstimate(flops=1_000_000_000, bytes_accessed=3_000_000, transcendentals=0),
        compiler_params=pltpu.CompilerParams(vmem_limit_bytes=8 << 20),
        name="project",
    )(*operands)


def dispatch_kernel(
    place_ref, tokens_ref, gain_ref, group_ref, expert_ref, routes_ref, k_ref, v_ref, order_ref, tail_ref, *send_refs
):
    tail_ref[...] = jnp.concatenate([k_ref[...], v_ref[...]], axis=0)
    groups = group_ref.shape[0]
    experts = expert_ref.shape[0]
    size = experts // groups
    rows, width = tokens_ref.shape
    values = tokens_ref[...].astype(jnp.float32)
    scaled = values * lax.rsqrt(jnp.mean(values * values, axis=-1, keepdims=True) + 1e-06) * gain_ref[...]
    normed = scaled.astype(jnp.bfloat16)
    group_logits = dot_f32(group_ref[...], normed, (1, 1))
    expert_logits = dot_f32(expert_ref[...], normed, (1, 1))
    first = routes_ref[0:1, :]
    second = routes_ref[1:2, :]
    group_index = lax.broadcasted_iota(jnp.int32, (groups, rows), 0)
    in_group = (first >= group_index * size) & (first < (group_index + 1) * size)
    group_exp = jnp.exp(group_logits - jnp.max(group_logits, axis=0, keepdims=True))
    share = jnp.sum(jnp.where(in_group, group_exp, 0.0), axis=0, keepdims=True) / jnp.sum(
        group_exp, axis=0, keepdims=True
    )
    expert_index = lax.broadcasted_iota(jnp.int32, (experts, rows), 0)
    pick_first = jnp.sum(jnp.where(expert_index == first, expert_logits, 0.0), axis=0, keepdims=True)
    pick_second = jnp.sum(jnp.where(expert_index == second, expert_logits, 0.0), axis=0, keepdims=True)
    pick_max = jnp.maximum(pick_first, pick_second)
    exp_first = jnp.exp(pick_first - pick_max)
    exp_second = jnp.exp(pick_second - pick_max)
    pick_sum = exp_first + exp_second
    gate_first = share * (exp_first / pick_sum)
    gate_second = share * (exp_second / pick_sum)
    earlier = lax.broadcasted_iota(jnp.int32, (rows, rows), 0) < lax.broadcasted_iota(jnp.int32, (rows, rows), 1)
    member = jnp.where(in_group, 1.0, 0.0)
    rank = dot_f32(member.astype(jnp.bfloat16), jnp.where(earlier, 1.0, 0.0).astype(jnp.bfloat16), (1, 0))
    chunk = (group_index ^ place_ref[2]) * (rows // groups)
    slot = jnp.sum(member * (chunk.astype(jnp.float32) + rank), axis=0, keepdims=True).astype(jnp.int32)
    order = jnp.where(lax.broadcasted_iota(jnp.int32, (rows, rows), 0) == slot, 1.0, 0.0).astype(jnp.bfloat16)
    order_ref[...] = order
    base = jnp.sum(jnp.where(in_group, group_index * size, 0), axis=0, keepdims=True)
    line = lax.broadcasted_iota(jnp.int32, (LANES, rows), 0)
    local = jnp.where(line < size, line, line - size) + base
    gate = jnp.where(local == first, gate_first, 0.0) + jnp.where(local == second, gate_second, 0.0)
    high = gate.astype(jnp.bfloat16).astype(jnp.float32)
    columns = jnp.where(line < size, high, jnp.where(line < 2 * size, gate - high, 0.0)).astype(jnp.bfloat16)
    moved = dot_f32(order, normed, (1, 0)).astype(jnp.bfloat16)
    moved_gates = dot_f32(order, columns, (1, 1)).astype(jnp.bfloat16)
    step = rows // groups
    for k, send in enumerate(send_refs):
        send[:, :width] = moved[k * step : (k + 1) * step]
        send[:, width:] = moved_gates[k * step : (k + 1) * step]


def dispatch(place, tokens, gain, group_t, expert_t, routes_t, k_t, v_t, rows):
    width = tokens.shape[1]
    groups = group_t.shape[0]
    step = rows // groups
    last = k_t.shape[1] // WINDOW - 1
    whole = lambda shape: pl.BlockSpec(shape, lambda i, s: tuple(0 for _ in shape))
    return pl.pallas_call(
        dispatch_kernel,
        grid_spec=pltpu.PrefetchScalarGridSpec(
            num_scalar_prefetch=1,
            grid=(1,),
            in_specs=[
                pl.BlockSpec((rows, width), lambda i, s: (s[1], 0)),
                whole((1, width)),
                whole(group_t.shape),
                whole(expert_t.shape),
                pl.BlockSpec((2, rows), lambda i, s: (0, s[1])),
                pl.BlockSpec((k_t.shape[0], WINDOW), lambda i, s: (0, last)),
                pl.BlockSpec((v_t.shape[0], WINDOW), lambda i, s: (0, last)),
            ],
            out_specs=[whole((rows, rows)), whole((k_t.shape[0] + v_t.shape[0], WINDOW))] + [whole((step, width + LANES)) for _ in range(groups)],
        ),
        out_shape=[
            jax.ShapeDtypeStruct((rows, rows), jnp.bfloat16),
            jax.ShapeDtypeStruct((k_t.shape[0] + v_t.shape[0], WINDOW), jnp.bfloat16),
        ]
        + [jax.ShapeDtypeStruct((step, width + LANES), jnp.bfloat16) for _ in range(groups)],
        cost_estimate=pl.CostEstimate(flops=1_000_000_000, bytes_accessed=2_000_000, transcendentals=0),
        compiler_params=pltpu.CompilerParams(vmem_limit_bytes=12 << 20),
        name="dispatch",
    )(place, *in_hbm(tokens, gain.reshape(1, width), group_t, expert_t, routes_t, k_t, v_t))


def experts_kernel(place_ref, *refs, sizes, size):
    count = len(sizes)
    pieces = refs[:count]
    gate_ref, up_ref, down_ref, out_ref, rows_ref = refs[count:]
    exp_local, width, hidden = gate_ref.shape
    at = 0
    for piece, rows in zip(pieces, sizes):
        rows_ref[at : at + rows, :] = piece[...]
        at += rows
    held = rows_ref[:, :width]
    gates = rows_ref[:, width:].astype(jnp.float32)
    line = lax.broadcasted_iota(jnp.int32, gates.shape, 1)
    active = []
    for e in range(exp_local):
        own = place_ref[3] * exp_local + e
        gate = jnp.sum(jnp.where((line == own) | (line == own + size), gates, 0.0), axis=1, keepdims=True)
        gate_pre = dot_f32(held, gate_ref[e], (1, 0))
        up_pre = dot_f32(held, up_ref[e], (1, 0))
        active.append((jax.nn.silu(gate_pre) * up_pre * gate).astype(jnp.bfloat16))
    down = down_ref[...].reshape(exp_local * hidden, width)
    out_ref[...] = dot_f32(jnp.concatenate(active, axis=1), down, (1, 0)).astype(jnp.bfloat16)


def run_experts(place, pieces, expert_gate, expert_up, expert_down, size):
    sizes = tuple(piece.shape[0] for piece in pieces)
    rows = sum(sizes)
    width = expert_gate.shape[1]
    vmem = pl.BlockSpec(memory_space=pltpu.VMEM)
    smem = pl.BlockSpec(memory_space=pltpu.SMEM)
    return pl.pallas_call(
        functools.partial(experts_kernel, sizes=sizes, size=size),
        out_shape=vmem_out((rows, width)),
        in_specs=[smem] + [vmem] * (len(pieces) + 3),
        out_specs=vmem,
        scratch_shapes=[pltpu.VMEM((rows, width + LANES), jnp.bfloat16)],
        cost_estimate=pl.CostEstimate(flops=rows * 7_000_000, bytes_accessed=15_000_000, transcendentals=0),
        compiler_params=pltpu.CompilerParams(vmem_limit_bytes=14 << 20),
        name="experts",
    )(place, *in_vmem(*pieces, expert_gate, expert_up, expert_down))


def combine_kernel(order_ref, *refs, steps):
    *pieces, out_ref, tile_ref, sems = refs
    rows = jnp.concatenate([piece[...] for piece in pieces], axis=0)
    width = rows.shape[1] // steps
    copies = []
    for i in range(steps):
        tile_ref[i] = dot_f32(order_ref[...], rows[:, i * width : (i + 1) * width], (0, 0)).astype(jnp.bfloat16)
        copies.append(
            pltpu.make_async_copy(tile_ref.at[i], out_ref.at[:, pl.ds(i * width, width)], sems.at[i])
        )
        copies[-1].start()
    for copy in copies:
        copy.wait()


def combine(order, pieces):
    vmem = pl.BlockSpec(memory_space=pltpu.VMEM)
    rows, width, steps = order.shape[0], pieces[0].shape[1], 4
    return pl.pallas_call(
        functools.partial(combine_kernel, steps=steps),
        out_shape=pltpu.HBM((rows, width), jnp.bfloat16),
        in_specs=[vmem] * (len(pieces) + 1),
        out_specs=pl.BlockSpec(memory_space=pl.ANY),
        scratch_shapes=[
            pltpu.VMEM((steps, rows, width // steps), jnp.bfloat16),
            pltpu.SemaphoreType.DMA((steps,)),
        ],
        compiler_params=pltpu.CompilerParams(vmem_limit_bytes=8 << 20),
        name="combine",
    )(*in_vmem(order, *pieces))


def sums_kernel(*refs, plan):
    values, outs = refs[: len(refs) - len(plan)], refs[len(refs) - len(plan) :]
    for out, segments in zip(outs, plan):
        for at, rows, terms in segments:
            parts = [values[i][start : start + rows, :].astype(jnp.float32) for i, start in terms]
            out[at : at + rows, :] = functools.reduce(jnp.add, parts).astype(jnp.bfloat16)


def sums(plan, *values):
    vmem = pl.BlockSpec(memory_space=pltpu.VMEM)
    width = values[0].shape[1]
    return pl.pallas_call(
        functools.partial(sums_kernel, plan=plan),
        out_shape=[vmem_out((sum(rows for _, rows, _ in segments), width)) for segments in plan],
        in_specs=[vmem] * len(values),
        out_specs=[vmem] * len(plan),
        compiler_params=pltpu.CompilerParams(vmem_limit_bytes=4 << 20),
        name="sums",
    )(*in_vmem(*values))


def gather_plane(own, core_bit, side_bit):
    half = own.shape[0] // 2
    across = flipped(own, "tp", side_bit)
    along = flipped(own, "ep", 1)
    far_low = flipped(across[:half], "ep", 1)
    far_high = flipped(along[half:], "tp", side_bit)
    ours = [own, across, along, far_low, far_high]
    return ours, [flipped(piece, "tp", core_bit) for piece in ours]


def reduce_plane(here, there, core_bit, side_bit, chunks):
    step = here.shape[0] // 4
    half = step // 2
    other = flipped(there, "tp", core_bit)
    both = lambda at: ((0, at), (1, at))
    first_side, first_along = sums(
        (
            ((0, half, both(3 * step + half)), (half, half, both(step + half))),
            ((0, half, both(3 * step)), (half, half, both(2 * step))),
        ),
        here,
        other,
    )
    first_side = flipped(first_side, "tp", side_bit)
    first_along = flipped(first_along, "ep", 1)
    second_side, second_along = sums(
        (((0, half, both(step) + ((2, 0),)),), ((0, half, both(2 * step + half) + ((3, 0),)),)),
        here,
        other,
        first_along,
        first_side,
    )
    second_side = flipped(second_side, "tp", side_bit)
    second_along = flipped(second_along, "ep", 1)
    piece = step // chunks
    plan = []
    for at in range(0, step, piece):
        if at < half:
            far = ((2, at), (5, half + at))
        else:
            far = ((4, at), (3, at - half))
        plan.append(((0, piece, both(at) + far),))
    return sums(tuple(plan), here, other, second_side, second_along, first_side, first_along)


def per_device(
    q_heads,
    k_heads,
    v_heads,
    sink_logits,
    out_weight,
    tokens_b,
    moe_gain,
    router_group,
    router_expert,
    route_expert,
    expert_gate,
    expert_up,
    expert_down,
):
    tp_count = lax.axis_size("tp")
    ep_count = lax.axis_size("ep")
    groups = router_group.shape[1]
    experts = router_expert.shape[1]
    exp_local = expert_gate.shape[0]
    members = ep_count // groups
    size = experts // groups
    rows_dev = tokens_b.shape[0] // tp_count
    capacity = min(4 * rows_dev // experts, rows_dev // 4)
    by_group = (
        tp_count == 4
        and members == 2
        and groups & (groups - 1) == 0
        and members * exp_local == size
        and rows_dev // groups <= exp_local * capacity
    )
    ep_index = lax.axis_index("ep")
    tp_index = lax.axis_index("tp")
    place = jnp.stack([ep_index, tp_index, ep_index // members, ep_index % members]).astype(jnp.int32)

    k_t = k_heads.T
    v_t = v_heads.T
    blocks = k_heads.shape[0] // WINDOW
    last = k_heads.shape[0] - WINDOW

    if not by_group:
        halo = shifted(jnp.concatenate([k_t[:, last:], v_t[:, last:]], axis=0), "ep", 1)
        attended = attend(place, q_heads, k_t, v_t, sink_logits, 0, blocks, [halo])
        mixed = jnp.dot(
            lax.all_gather(attended, "tp", axis=1, tiled=True), out_weight, preferred_element_type=jnp.float32
        )
        return (
            mixed.astype(jnp.bfloat16),
            moe_by_slot(
                tokens_b, moe_gain, router_group, router_expert, route_expert, expert_gate, expert_up, expert_down
            ),
        )

    core_bit, side_bit = 1, 2
    order, tail, *sends = dispatch(
        place, tokens_b, moe_gain, router_group.T, router_expert.T, route_expert.T, k_t, v_t, rows_dev
    )
    halo = shifted(tail, "ep", 1)
    chunks = ((0, 3), (1, 2)) if groups == 4 else (tuple(range(groups)),)
    arrived = [sends[0]] + [flipped(sends[k], "ep", k * members) for k in range(1, groups)]
    middle = blocks // 2
    attended = []
    for first, end in ((0, middle), (middle, blocks)):
        attended.append(attend(place, q_heads, k_t, v_t, sink_logits, first, end, [halo] if first == 0 else []))
    results = []
    for chunk in chunks:
        own = jnp.concatenate([arrived[k] for k in chunk], axis=0)
        halves = []
        for pieces in gather_plane(own, core_bit, side_bit):
            halves.append(run_experts(place, pieces, expert_gate, expert_up, expert_down, size))
        results.append(halves)
    core = [flipped(part, "tp", core_bit) for part in attended]
    side = [flipped(part, "tp", side_bit) for part in attended]
    cross = [flipped(part, "tp", core_bit) for part in side]
    held = []
    for part in reversed(range(len(attended))):
        pieces = [attended[part], core[part], side[part], cross[part]]
        held = [project(place, pieces, out_weight, part, len(attended), held)]
    (mixer_out,) = held
    returned = {}
    for chunk, (here, there) in zip(chunks, results):
        totals = reduce_plane(here, there, core_bit, side_bit, len(chunk))
        for k, total in zip(chunk, totals):
            returned[k] = flipped(total, "ep", k * members) if k else total
    moe_out = combine(order, [returned[k] for k in range(groups)])
    return (mixer_out, moe_out)


def normalize(rows_in, gain):
    values = rows_in.astype(jnp.float32)
    scaled = values * lax.rsqrt(jnp.mean(values * values, axis=-1, keepdims=True) + 1e-06) * gain
    return scaled.astype(jnp.bfloat16)


def gate_weights(normed, routes, router_group, router_expert):
    group_logits = jnp.dot(normed, router_group, preferred_element_type=jnp.float32)
    expert_logits = jnp.dot(normed, router_expert, preferred_element_type=jnp.float32)
    group_count = router_group.shape[1]
    expert_count = router_expert.shape[1]
    chosen_group = routes[:, 0] // (expert_count // group_count)
    group_match = chosen_group[:, None] == jnp.arange(group_count, dtype=jnp.int32)[None, :]
    group_share = jnp.sum(jnp.where(group_match, jax.nn.softmax(group_logits, axis=-1), 0.0), axis=-1)
    expert_match = routes[:, :, None] == jnp.arange(expert_count, dtype=jnp.int32)[None, None, :]
    picked = jnp.sum(jnp.where(expert_match, expert_logits[:, None, :], 0.0), axis=-1)
    return group_share[:, None] * jax.nn.softmax(picked, axis=-1)


def moe_by_slot(
    tokens_b, moe_gain, router_group, router_expert, route_expert, expert_gate, expert_up, expert_down
):
    tp_count = lax.axis_size("tp")
    tp_index = lax.axis_index("tp")
    exp_local = expert_gate.shape[0]
    expert_count = exp_local * lax.axis_size("ep")
    rows_dev = tokens_b.shape[0] // tp_count
    width = tokens_b.shape[1]
    capacity = min(4 * rows_dev // expert_count, rows_dev // 4)
    routes = lax.dynamic_slice_in_dim(route_expert, tp_index * rows_dev, rows_dev, 0)
    normed = normalize(lax.dynamic_slice_in_dim(tokens_b, tp_index * rows_dev, rows_dev, 0), moe_gain)
    flat_routes = routes.reshape(-1)
    onehot = (flat_routes[:, None] == jnp.arange(expert_count, dtype=jnp.int32)[None, :]).astype(jnp.int32)
    places = jnp.sum(onehot * jnp.cumsum(onehot, axis=0), axis=1) - 1
    target = flat_routes * capacity + places
    buffer = jnp.zeros((expert_count * capacity, width), jnp.bfloat16)
    buffer = buffer.at[target].set(jnp.repeat(normed, 2, axis=0))
    buffer = buffer.reshape(expert_count // exp_local, exp_local, 1, capacity, width)
    delivered = lax.all_to_all(buffer, "ep", split_axis=0, concat_axis=0, tiled=True)
    arrived = lax.all_gather(delivered, "tp", axis=2, tiled=True)
    gates = gate_weights(normed, routes, router_group, router_expert)
    gate_pre = jnp.einsum("setcd,edf->setcf", arrived, expert_gate, preferred_element_type=jnp.float32)
    up_pre = jnp.einsum("setcd,edf->setcf", arrived, expert_up, preferred_element_type=jnp.float32)
    activated = (jax.nn.silu(gate_pre) * up_pre).astype(jnp.bfloat16)
    partial_value = jnp.einsum("setcf,efd->setcd", activated, expert_down, preferred_element_type=jnp.float32)
    summed = lax.psum_scatter(partial_value.astype(jnp.bfloat16), "tp", scatter_dimension=2, tiled=True)
    returned = lax.all_to_all(summed, "ep", split_axis=0, concat_axis=0, tiled=True)
    picked_rows = returned.reshape(expert_count * capacity, width)[target].reshape(rows_dev, 2, width)
    return jnp.sum(gates[:, :, None] * picked_rows.astype(jnp.float32), axis=1).astype(jnp.bfloat16)


def solution(mesh):
    in_specs = (
        P("ep", "tp"),
        P("ep", "tp"),
        P("ep", "tp"),
        P("tp"),
        P(None, "tp"),
        P("ep", None),
        P(),
        P(),
        P(),
        P("ep", None),
        P("ep", None, "tp"),
        P("ep", None, "tp"),
        P("ep", "tp", None),
    )
    out_specs = (P("ep", "tp"), P(("ep", "tp"), None))

    return jax.shard_map(per_device, mesh=mesh, in_specs=in_specs, out_specs=out_specs, check_vma=False)
```

```python
import functools

import jax
import jax.numpy as jnp
from jax import lax
from jax.experimental import pallas as pl
from jax.experimental.pallas import tpu as pltpu
from jax.sharding import PartitionSpec as P


HEADS = 16
KV = 4
HD = 64
WINDOW = 128
LANES = 128


def shifted(value, axis, steps):
    count = lax.axis_size(axis)
    leading, last = (max(0, -steps), min(count, count - steps))
    return lax.ppermute(value, axis, [(source, source + steps) for source in range(leading, last)])


def flipped(value, axis, bits):
    return lax.ppermute(value, axis, [(i, i ^ bits) for i in range(lax.axis_size(axis))])


def in_vmem(*values):
    return [pltpu.with_memory_space_constraint(v, pltpu.VMEM) for v in values]


def in_hbm(*values):
    return [pltpu.with_memory_space_constraint(v, pltpu.HBM) for v in values]


def vmem_out(shape, dtype=jnp.bfloat16):
    return pltpu.VMEM(shape, dtype)


def dot_f32(a, b, contract):
    return lax.dot_general(a, b, ((contract[:1], contract[1:]), ((), ())), preferred_element_type=jnp.float32)


def attention_kernel(place_ref, q_ref, kt_ref, vt_ref, sink_ref, *refs, first, kv_local, group_size):
    *halo, out_ref = refs
    span = WINDOW
    query_index = lax.broadcasted_iota(jnp.int32, (span, 2 * span), 0)
    key_index = lax.broadcasted_iota(jnp.int32, (span, 2 * span), 1)
    banded = (key_index > query_index) & (key_index <= query_index + span)
    half = kv_local * HD
    for block in range(out_ref.shape[0] // span):
        here = pl.ds((first + block) * span, span)
        band = pl.ds((first + block - 1) * span, 2 * span)
        at_start = first + block == 0
        allowed = banded & ((key_index >= span) | (place_ref[0] > 0)) if at_start else banded
        for kv in range(kv_local):
            heads = pl.ds(kv * HD, HD)
            if at_start:
                (halo_ref,) = halo
                k_band = jnp.concatenate([halo_ref[kv * HD : (kv + 1) * HD, :], kt_ref[heads, here]], axis=1)
                v_band = jnp.concatenate(
                    [halo_ref[half + kv * HD : half + (kv + 1) * HD, :], vt_ref[heads, here]], axis=1
                )
            else:
                k_band = kt_ref[heads, band]
                v_band = vt_ref[heads, band]
            mixed = []
            for member in range(group_size):
                head = kv * group_size + member
                scores = dot_f32(q_ref[here, pl.ds(head * HD, HD)], k_band, (1, 0)) * HD ** (-0.5)
                masked = jnp.where(allowed, scores, -1e30)
                sink = sink_ref[head]
                row_max = jnp.maximum(jnp.max(masked, axis=1, keepdims=True), sink)
                weights_exp = jnp.exp(masked - row_max)
                denominator = jnp.sum(weights_exp, axis=1, keepdims=True) + jnp.exp(sink - row_max)
                probs = (weights_exp * (1.0 / denominator)).astype(jnp.bfloat16)
                mixed.append(dot_f32(probs, v_band, (1, 1)))
            out_ref[block * span : (block + 1) * span, pl.ds(kv * group_size * HD, group_size * HD)] = (
                jnp.concatenate(mixed, axis=1).astype(jnp.bfloat16)
            )


def attend(place, q_heads, k_t, v_t, sink_logits, first, last, halo):
    kv_local = k_t.shape[0] // HD
    vmem = pl.BlockSpec(memory_space=pltpu.VMEM)
    smem = pl.BlockSpec(memory_space=pltpu.SMEM)
    return pl.pallas_call(
        functools.partial(attention_kernel, first=first, kv_local=kv_local, group_size=HEADS // KV),
        out_shape=jax.ShapeDtypeStruct(((last - first) * WINDOW, q_heads.shape[1]), jnp.bfloat16),
        in_specs=[smem, vmem, vmem, vmem, smem] + [vmem] * len(halo),
        out_specs=vmem,
        cost_estimate=pl.CostEstimate(flops=3_000_000_000, bytes_accessed=2_000_000, transcendentals=0),
        compiler_params=pltpu.CompilerParams(vmem_limit_bytes=12 << 20),
        name="attend",
    )(place, q_heads, k_t, v_t, sink_logits, *halo)


def projection_kernel(place_ref, *refs, count, first, steps):
    pieces, weight_ref = refs[:count], refs[count]
    out_ref, tile_ref, sems = refs[-3:]
    rows, width = pieces[0].shape
    tile = rows // steps
    copies = []
    for i in range(steps):
        total = None
        for bits, piece in enumerate(pieces):
            lines = pl.ds(pl.multiple_of((place_ref[1] ^ bits) * width, width), width)
            product = dot_f32(piece[i * tile : (i + 1) * tile, :], weight_ref[lines, :], (1, 0))
            total = product if total is None else total + product
        tile_ref[i] = total.astype(jnp.bfloat16)
        copies.append(
            pltpu.make_async_copy(tile_ref.at[i], out_ref.at[pl.ds(first + i * tile, tile), :], sems.at[i])
        )
        copies[-1].start()
    for copy in copies:
        copy.wait()


def project(place, pieces, out_weight, part, parts, held):
    rows = pieces[0].shape[0]
    steps = 1
    vmem = pl.BlockSpec(memory_space=pltpu.VMEM)
    operands = [place, *in_vmem(*pieces, out_weight), *held]
    return pl.pallas_call(
        functools.partial(projection_kernel, count=len(pieces), first=part * rows, steps=steps),
        in_specs=[pl.BlockSpec(memory_space=pltpu.SMEM)]
        + [vmem] * (len(pieces) + 1)
        + [pl.BlockSpec(memory_space=pl.ANY) for _ in held],
        out_specs=pl.BlockSpec(memory_space=pl.ANY),
        out_shape=pltpu.HBM((rows * parts, out_weight.shape[1]), jnp.bfloat16),
        scratch_shapes=[
            pltpu.VMEM((steps, rows // steps, out_weight.shape[1]), jnp.bfloat16),
            pltpu.SemaphoreType.DMA((steps,)),
        ],
        input_output_aliases={len(operands) - 1: 0} if held else {},
        cost_estimate=pl.CostEstimate(flops=1_000_000_000, bytes_accessed=3_000_000, transcendentals=0),
        compiler_params=pltpu.CompilerParams(vmem_limit_bytes=8 << 20),
        name="project",
    )(*operands)


def dispatch_kernel(
    place_ref, tokens_ref, gain_ref, group_ref, expert_ref, routes_ref, k_ref, v_ref, order_ref, tail_ref, *send_refs
):
    tail_ref[...] = jnp.concatenate([k_ref[...], v_ref[...]], axis=0)
    groups = group_ref.shape[0]
    experts = expert_ref.shape[0]
    size = experts // groups
    rows, width = tokens_ref.shape
    values = tokens_ref[...].astype(jnp.float32)
    scaled = values * lax.rsqrt(jnp.mean(values * values, axis=-1, keepdims=True) + 1e-06) * gain_ref[...]
    normed = scaled.astype(jnp.bfloat16)
    logits = dot_f32(jnp.concatenate([expert_ref[...], group_ref[...]], axis=0), normed, (1, 1))
    expert_logits = logits[:experts]
    group_logits = logits[experts:]
    first = routes_ref[0:1, :]
    second = routes_ref[1:2, :]
    group_index = lax.broadcasted_iota(jnp.int32, (groups, rows), 0)
    in_group = (first >= group_index * size) & (first < (group_index + 1) * size)
    group_exp = jnp.exp(group_logits - jnp.max(group_logits, axis=0, keepdims=True))
    share = jnp.sum(jnp.where(in_group, group_exp, 0.0), axis=0, keepdims=True) / jnp.sum(
        group_exp, axis=0, keepdims=True
    )
    expert_index = lax.broadcasted_iota(jnp.int32, (experts, rows), 0)
    pick_first = jnp.sum(jnp.where(expert_index == first, expert_logits, 0.0), axis=0, keepdims=True)
    pick_second = jnp.sum(jnp.where(expert_index == second, expert_logits, 0.0), axis=0, keepdims=True)
    pick_max = jnp.maximum(pick_first, pick_second)
    exp_first = jnp.exp(pick_first - pick_max)
    exp_second = jnp.exp(pick_second - pick_max)
    pick_sum = exp_first + exp_second
    gate_first = share * (exp_first / pick_sum)
    gate_second = share * (exp_second / pick_sum)
    earlier = lax.broadcasted_iota(jnp.int32, (rows, rows), 0) < lax.broadcasted_iota(jnp.int32, (rows, rows), 1)
    member = jnp.where(in_group, 1.0, 0.0)
    rank = dot_f32(member.astype(jnp.bfloat16), jnp.where(earlier, 1.0, 0.0).astype(jnp.bfloat16), (1, 0))
    chunk = (group_index ^ place_ref[2]) * (rows // groups)
    slot = jnp.sum(member * (chunk.astype(jnp.float32) + rank), axis=0, keepdims=True).astype(jnp.int32)
    order = jnp.where(lax.broadcasted_iota(jnp.int32, (rows, rows), 0) == slot, 1.0, 0.0).astype(jnp.bfloat16)
    order_ref[...] = order
    base = jnp.sum(jnp.where(in_group, group_index * size, 0), axis=0, keepdims=True)
    line = lax.broadcasted_iota(jnp.int32, (LANES, rows), 0)
    local = jnp.where(line < size, line, line - size) + base
    gate = jnp.where(local == first, gate_first, 0.0) + jnp.where(local == second, gate_second, 0.0)
    high = gate.astype(jnp.bfloat16).astype(jnp.float32)
    columns = jnp.where(line < size, high, jnp.where(line < 2 * size, gate - high, 0.0)).astype(jnp.bfloat16)
    moved = dot_f32(order, normed, (1, 0)).astype(jnp.bfloat16)
    moved_gates = dot_f32(order, columns, (1, 1)).astype(jnp.bfloat16)
    step = rows // groups
    for k, send in enumerate(send_refs):
        send[:, :width] = moved[k * step : (k + 1) * step]
        send[:, width:] = moved_gates[k * step : (k + 1) * step]


def dispatch(place, tokens, gain, group_t, expert_t, routes_t, k_t, v_t, rows):
    width = tokens.shape[1]
    groups = group_t.shape[0]
    step = rows // groups
    last = k_t.shape[1] // WINDOW - 1
    whole = lambda shape: pl.BlockSpec(shape, lambda i, s: tuple(0 for _ in shape))
    return pl.pallas_call(
        dispatch_kernel,
        grid_spec=pltpu.PrefetchScalarGridSpec(
            num_scalar_prefetch=1,
            grid=(1,),
            in_specs=[
                pl.BlockSpec((rows, width), lambda i, s: (s[1], 0)),
                whole((1, width)),
                whole(group_t.shape),
                whole(expert_t.shape),
                pl.BlockSpec((2, rows), lambda i, s: (0, s[1])),
                pl.BlockSpec((k_t.shape[0], WINDOW), lambda i, s: (0, last)),
                pl.BlockSpec((v_t.shape[0], WINDOW), lambda i, s: (0, last)),
            ],
            out_specs=[whole((rows, rows)), whole((k_t.shape[0] + v_t.shape[0], WINDOW))] + [whole((step, width + LANES)) for _ in range(groups)],
        ),
        out_shape=[
            jax.ShapeDtypeStruct((rows, rows), jnp.bfloat16),
            jax.ShapeDtypeStruct((k_t.shape[0] + v_t.shape[0], WINDOW), jnp.bfloat16),
        ]
        + [jax.ShapeDtypeStruct((step, width + LANES), jnp.bfloat16) for _ in range(groups)],
        cost_estimate=pl.CostEstimate(flops=1_000_000_000, bytes_accessed=2_000_000, transcendentals=0),
        compiler_params=pltpu.CompilerParams(vmem_limit_bytes=12 << 20),
        name="dispatch",
    )(place, *in_hbm(tokens, gain.reshape(1, width), group_t, expert_t, routes_t, k_t, v_t))


def experts_kernel(place_ref, *refs, sizes, size):
    count = len(sizes)
    pieces = refs[:count]
    gate_ref, up_ref, down_ref, out_ref = refs[count:]
    exp_local, width, hidden = gate_ref.shape
    held = jnp.concatenate([piece[:, :width] for piece in pieces], axis=0)
    gates = jnp.concatenate([piece[:, width:] for piece in pieces], axis=0).astype(jnp.float32)
    line = lax.broadcasted_iota(jnp.int32, gates.shape, 1)
    active = []
    for e in range(exp_local):
        own = place_ref[3] * exp_local + e
        gate = jnp.sum(jnp.where((line == own) | (line == own + size), gates, 0.0), axis=1, keepdims=True)
        gate_pre = dot_f32(held, gate_ref[e], (1, 0))
        up_pre = dot_f32(held, up_ref[e], (1, 0))
        active.append((jax.nn.silu(gate_pre) * up_pre * gate).astype(jnp.bfloat16))
    down = down_ref[...].reshape(exp_local * hidden, width)
    out_ref[...] = dot_f32(jnp.concatenate(active, axis=1), down, (1, 0)).astype(jnp.bfloat16)


def run_experts(place, pieces, expert_gate, expert_up, expert_down, size):
    sizes = tuple(piece.shape[0] for piece in pieces)
    rows = sum(sizes)
    width = expert_gate.shape[1]
    vmem = pl.BlockSpec(memory_space=pltpu.VMEM)
    smem = pl.BlockSpec(memory_space=pltpu.SMEM)
    return pl.pallas_call(
        functools.partial(experts_kernel, sizes=sizes, size=size),
        out_shape=vmem_out((rows, width)),
        in_specs=[smem] + [vmem] * (len(pieces) + 3),
        out_specs=vmem,
        cost_estimate=pl.CostEstimate(flops=rows * 7_000_000, bytes_accessed=15_000_000, transcendentals=0),
        compiler_params=pltpu.CompilerParams(vmem_limit_bytes=14 << 20),
        name="experts",
    )(place, *in_vmem(*pieces, expert_gate, expert_up, expert_down))


def combine_kernel(order_ref, *refs, steps):
    *pieces, out_ref, tile_ref, sems = refs
    rows = jnp.concatenate([piece[...] for piece in pieces], axis=0)
    width = rows.shape[1] // steps
    copies = []
    for i in range(steps):
        tile_ref[i] = dot_f32(order_ref[...], rows[:, i * width : (i + 1) * width], (0, 0)).astype(jnp.bfloat16)
        copies.append(
            pltpu.make_async_copy(tile_ref.at[i], out_ref.at[:, pl.ds(i * width, width)], sems.at[i])
        )
        copies[-1].start()
    for copy in copies:
        copy.wait()


def combine(order, pieces):
    vmem = pl.BlockSpec(memory_space=pltpu.VMEM)
    rows, width, steps = order.shape[0], pieces[0].shape[1], 4
    return pl.pallas_call(
        functools.partial(combine_kernel, steps=steps),
        out_shape=pltpu.HBM((rows, width), jnp.bfloat16),
        in_specs=[vmem] * (len(pieces) + 1),
        out_specs=pl.BlockSpec(memory_space=pl.ANY),
        scratch_shapes=[
            pltpu.VMEM((steps, rows, width // steps), jnp.bfloat16),
            pltpu.SemaphoreType.DMA((steps,)),
        ],
        compiler_params=pltpu.CompilerParams(vmem_limit_bytes=8 << 20),
        name="combine",
    )(*in_vmem(order, *pieces))


def sums_kernel(*refs, plan):
    values, outs = refs[: len(refs) - len(plan)], refs[len(refs) - len(plan) :]
    for out, segments in zip(outs, plan):
        for at, rows, terms in segments:
            parts = [values[i][start : start + rows, :].astype(jnp.float32) for i, start in terms]
            out[at : at + rows, :] = functools.reduce(jnp.add, parts).astype(jnp.bfloat16)


def sums(plan, *values):
    vmem = pl.BlockSpec(memory_space=pltpu.VMEM)
    width = values[0].shape[1]
    return pl.pallas_call(
        functools.partial(sums_kernel, plan=plan),
        out_shape=[vmem_out((sum(rows for _, rows, _ in segments), width)) for segments in plan],
        in_specs=[vmem] * len(values),
        out_specs=[vmem] * len(plan),
        compiler_params=pltpu.CompilerParams(vmem_limit_bytes=4 << 20),
        name="sums",
    )(*in_vmem(*values))


def gather_plane(own, core_bit, side_bit):
    half = own.shape[0] // 2
    across = flipped(own, "tp", side_bit)
    along = flipped(own, "ep", 1)
    far_low = flipped(across[:half], "ep", 1)
    far_high = flipped(along[half:], "tp", side_bit)
    ours = [own, across, along, far_low, far_high]
    return ours, [flipped(piece, "tp", core_bit) for piece in ours]


def reduce_plane(here, there, core_bit, side_bit, chunks):
    step = here.shape[0] // 4
    half = step // 2
    other = flipped(there, "tp", core_bit)
    both = lambda at: ((0, at), (1, at))
    first_side, first_along = sums(
        (
            ((0, half, both(3 * step + half)), (half, half, both(step + half))),
            ((0, half, both(3 * step)), (half, half, both(2 * step))),
        ),
        here,
        other,
    )
    first_side = flipped(first_side, "tp", side_bit)
    first_along = flipped(first_along, "ep", 1)
    second_side, second_along = sums(
        (((0, half, both(step) + ((2, 0),)),), ((0, half, both(2 * step + half) + ((3, 0),)),)),
        here,
        other,
        first_along,
        first_side,
    )
    second_side = flipped(second_side, "tp", side_bit)
    second_along = flipped(second_along, "ep", 1)
    piece = step // chunks
    plan = []
    for at in range(0, step, piece):
        if at < half:
            far = ((2, at), (5, half + at))
        else:
            far = ((4, at), (3, at - half))
        plan.append(((0, piece, both(at) + far),))
    return sums(tuple(plan), here, other, second_side, second_along, first_side, first_along)


def per_device(
    q_heads,
    k_heads,
    v_heads,
    sink_logits,
    out_weight,
    tokens_b,
    moe_gain,
    router_group,
    router_expert,
    route_expert,
    expert_gate,
    expert_up,
    expert_down,
):
    tp_count = lax.axis_size("tp")
    ep_count = lax.axis_size("ep")
    groups = router_group.shape[1]
    experts = router_expert.shape[1]
    exp_local = expert_gate.shape[0]
    members = ep_count // groups
    size = experts // groups
    rows_dev = tokens_b.shape[0] // tp_count
    capacity = min(4 * rows_dev // experts, rows_dev // 4)
    by_group = (
        tp_count == 4
        and members == 2
        and groups & (groups - 1) == 0
        and members * exp_local == size
        and rows_dev // groups <= exp_local * capacity
    )
    ep_index = lax.axis_index("ep")
    tp_index = lax.axis_index("tp")
    place = jnp.stack([ep_index, tp_index, ep_index // members, ep_index % members]).astype(jnp.int32)

    k_t = k_heads.T
    v_t = v_heads.T
    blocks = k_heads.shape[0] // WINDOW
    last = k_heads.shape[0] - WINDOW

    if not by_group:
        halo = shifted(jnp.concatenate([k_t[:, last:], v_t[:, last:]], axis=0), "ep", 1)
        attended = attend(place, q_heads, k_t, v_t, sink_logits, 0, blocks, [halo])
        mixed = jnp.dot(
            lax.all_gather(attended, "tp", axis=1, tiled=True), out_weight, preferred_element_type=jnp.float32
        )
        return (
            mixed.astype(jnp.bfloat16),
            moe_by_slot(
                tokens_b, moe_gain, router_group, router_expert, route_expert, expert_gate, expert_up, expert_down
            ),
        )

    core_bit, side_bit = 1, 2
    order, tail, *sends = dispatch(
        place, tokens_b, moe_gain, router_group.T, router_expert.T, route_expert.T, k_t, v_t, rows_dev
    )
    halo = shifted(tail, "ep", 1)
    chunks = ((0, 3), (1, 2)) if groups == 4 else (tuple(range(groups)),)
    arrived = [sends[0]] + [flipped(sends[k], "ep", k * members) for k in range(1, groups)]
    middle = blocks // 2
    attended = []
    for first, end in ((0, middle), (middle, blocks)):
        attended.append(attend(place, q_heads, k_t, v_t, sink_logits, first, end, [halo] if first == 0 else []))
    results = []
    for chunk in chunks:
        own = jnp.concatenate([arrived[k] for k in chunk], axis=0)
        halves = []
        for pieces in gather_plane(own, core_bit, side_bit):
            halves.append(run_experts(place, pieces, expert_gate, expert_up, expert_down, size))
        results.append(halves)
    core = [flipped(part, "tp", core_bit) for part in attended]
    side = [flipped(part, "tp", side_bit) for part in attended]
    cross = [flipped(part, "tp", core_bit) for part in side]
    held = []
    for part in reversed(range(len(attended))):
        pieces = [attended[part], core[part], side[part], cross[part]]
        held = [project(place, pieces, out_weight, part, len(attended), held)]
    (mixer_out,) = held
    returned = {}
    for chunk, (here, there) in zip(chunks, results):
        totals = reduce_plane(here, there, core_bit, side_bit, len(chunk))
        for k, total in zip(chunk, totals):
            returned[k] = flipped(total, "ep", k * members) if k else total
    moe_out = combine(order, [returned[k] for k in range(groups)])
    return (mixer_out, moe_out)


def normalize(rows_in, gain):
    values = rows_in.astype(jnp.float32)
    scaled = values * lax.rsqrt(jnp.mean(values * values, axis=-1, keepdims=True) + 1e-06) * gain
    return scaled.astype(jnp.bfloat16)


def gate_weights(normed, routes, router_group, router_expert):
    group_logits = jnp.dot(normed, router_group, preferred_element_type=jnp.float32)
    expert_logits = jnp.dot(normed, router_expert, preferred_element_type=jnp.float32)
    group_count = router_group.shape[1]
    expert_count = router_expert.shape[1]
    chosen_group = routes[:, 0] // (expert_count // group_count)
    group_match = chosen_group[:, None] == jnp.arange(group_count, dtype=jnp.int32)[None, :]
    group_share = jnp.sum(jnp.where(group_match, jax.nn.softmax(group_logits, axis=-1), 0.0), axis=-1)
    expert_match = routes[:, :, None] == jnp.arange(expert_count, dtype=jnp.int32)[None, None, :]
    picked = jnp.sum(jnp.where(expert_match, expert_logits[:, None, :], 0.0), axis=-1)
    return group_share[:, None] * jax.nn.softmax(picked, axis=-1)


def moe_by_slot(
    tokens_b, moe_gain, router_group, router_expert, route_expert, expert_gate, expert_up, expert_down
):
    tp_count = lax.axis_size("tp")
    tp_index = lax.axis_index("tp")
    exp_local = expert_gate.shape[0]
    expert_count = exp_local * lax.axis_size("ep")
    rows_dev = tokens_b.shape[0] // tp_count
    width = tokens_b.shape[1]
    capacity = min(4 * rows_dev // expert_count, rows_dev // 4)
    routes = lax.dynamic_slice_in_dim(route_expert, tp_index * rows_dev, rows_dev, 0)
    normed = normalize(lax.dynamic_slice_in_dim(tokens_b, tp_index * rows_dev, rows_dev, 0), moe_gain)
    flat_routes = routes.reshape(-1)
    onehot = (flat_routes[:, None] == jnp.arange(expert_count, dtype=jnp.int32)[None, :]).astype(jnp.int32)
    places = jnp.sum(onehot * jnp.cumsum(onehot, axis=0), axis=1) - 1
    target = flat_routes * capacity + places
    buffer = jnp.zeros((expert_count * capacity, width), jnp.bfloat16)
    buffer = buffer.at[target].set(jnp.repeat(normed, 2, axis=0))
    buffer = buffer.reshape(expert_count // exp_local, exp_local, 1, capacity, width)
    delivered = lax.all_to_all(buffer, "ep", split_axis=0, concat_axis=0, tiled=True)
    arrived = lax.all_gather(delivered, "tp", axis=2, tiled=True)
    gates = gate_weights(normed, routes, router_group, router_expert)
    gate_pre = jnp.einsum("setcd,edf->setcf", arrived, expert_gate, preferred_element_type=jnp.float32)
    up_pre = jnp.einsum("setcd,edf->setcf", arrived, expert_up, preferred_element_type=jnp.float32)
    activated = (jax.nn.silu(gate_pre) * up_pre).astype(jnp.bfloat16)
    partial_value = jnp.einsum("setcf,efd->setcd", activated, expert_down, preferred_element_type=jnp.float32)
    summed = lax.psum_scatter(partial_value.astype(jnp.bfloat16), "tp", scatter_dimension=2, tiled=True)
    returned = lax.all_to_all(summed, "ep", split_axis=0, concat_axis=0, tiled=True)
    picked_rows = returned.reshape(expert_count * capacity, width)[target].reshape(rows_dev, 2, width)
    return jnp.sum(gates[:, :, None] * picked_rows.astype(jnp.float32), axis=1).astype(jnp.bfloat16)


def solution(mesh):
    in_specs = (
        P("ep", "tp"),
        P("ep", "tp"),
        P("ep", "tp"),
        P("tp"),
        P(None, "tp"),
        P("ep", None),
        P(),
        P(),
        P(),
        P("ep", None),
        P("ep", None, "tp"),
        P("ep", None, "tp"),
        P("ep", "tp", None),
    )
    out_specs = (P("ep", "tp"), P(("ep", "tp"), None))

    return jax.shard_map(per_device, mesh=mesh, in_specs=in_specs, out_specs=out_specs, check_vma=False)
```
